256 devices in a mesh: grp: 4 (over y, x), sp: 32 (over z), tp: 2 (over core).
Axes of the slice: x: 2, y: 2, z: 32, core: 2. Of those that a mesh axis runs over, the one named last changes fastest.
The devices are a block of a 4x16x32 slice.
Arguments:
- tokens: bfloat16 [65536, 2048], P(('grp', 'sp', 'tp')), parts along dimension 0, may hold values from -60 to 60
- query_weight: bfloat16 [2048, 1024], P(None, 'tp'), may hold values from -0.125 to 0.125
- key_weight: bfloat16 [2048, 1024], P(None, 'tp'), may hold values from -0.125 to 0.125
- value_weight: bfloat16 [2048, 1024], P(None, 'tp'), may hold values from -0.125 to 0.125
- output_weight: bfloat16 [1024, 2048], P(None, 'tp'), may hold values from -1.5 to 1.5
Outputs:
- attended: bfloat16 [65536, 2048], P(('grp', 'sp'), 'tp'), parts along dimension 0
The draws below stay inside these ranges and needn't reach their ends.
There are 4 independent parts, one for each index of `grp`. The reference program is written for one: setup_inputs(seed, part) draws one part's arguments, and reference() takes and returns one part's arrays. A program takes and returns all parts, laid end to end along the dimension named above; an argument that names none is the same for every part. Nothing has to cross between parts.
All inputs are finite; a program needn't handle non-finite values.
Results may differ from the reference program's by a relative error of at most 0.012.
The reference program's roundings to bfloat16 on the way (of `queries`, `keys`, `values`, `weights` and `mixed`) count: a program that leaves them out, or rounds other values in their place, can miss the bound.
Values may be sent and summed in bfloat16 or wider, within the bound.
A program may use at most 128 MiB of HBM per device.

```python
import jax
import jax.numpy as jnp
from jax import lax

D = 2048
HEADS = 8
HEAD = 128
REACH_STEPS = 128
MIDDLE_DILATION = 4
FAR_DILATION = 16
TOKENS = 16384


def draw_tokens(key, part):
    key_base = jax.random.fold_in(key, 11)
    base = jnp.clip(jax.random.normal(key_base, (TOKENS, D), jnp.float32), -6.0, 6.0)
    return base.astype(jnp.bfloat16)


def steps_of(rng, shape, cuts, smallest, largest):
    gain, own = 1.0, jax.random.fold_in(rng, 6)
    for position, blocks in cuts:
        draws = jnp.exp(jax.random.uniform(jax.random.fold_in(own, position), (blocks,), jnp.float32, smallest / len(cuts), largest / len(cuts)))
        gain = gain * jnp.repeat(draws, shape[position] // blocks).reshape([-1 if axis == position else 1 for axis in range(len(shape))])
    return gain


def gaussian(key, extent, deviation, reach, shards=(), kind=jnp.bfloat16):
    factor_of = steps_of(key, extent, shards, -0.22, 0.18) if shards else 1.0
    entries = jax.random.normal(key, extent, jnp.float32) * deviation * factor_of
    return jnp.minimum(jnp.maximum(entries, -reach), reach).astype(kind)


def setup_inputs(seed: int = 0, part: int = 0) -> dict:
    key_of = jax.random.split(jax.random.key(seed), 6)
    own_keys = jax.random.split(jax.random.fold_in(key_of[5], part), 6)
    tokens = draw_tokens(jax.random.fold_in(jax.random.fold_in(key_of[5], part), 71), part)
    query_weight = gaussian(key_of[1], (D, HEADS * HEAD), D ** -0.5, 0.125, ((1, 2),))
    key_weight = gaussian(key_of[2], (D, HEADS * HEAD), D ** -0.5, 0.125, ((1, 2),))
    value_weight = gaussian(key_of[3], (D, HEADS * HEAD), D ** -0.5, 0.125, ((1, 2),))
    output_weight = gaussian(key_of[4], (HEADS * HEAD, D), (REACH_STEPS // 8) ** -0.5, 1.5, ((1, 2),))
    return dict(tokens=tokens, query_weight=query_weight, key_weight=key_weight, value_weight=value_weight, output_weight=output_weight)


THETA_BASE = 500000.0


def rotate(values, positions):
    half = values.shape[-1] // 2
    inverse = THETA_BASE ** (-jnp.arange(half, dtype=jnp.float32) / half)
    angles = positions[:, None, None] * inverse
    cosine = jnp.cos(angles)
    sine = jnp.sin(angles)
    first = values[..., :half]
    second = values[..., half:]
    return jnp.concatenate([first * cosine - second * sine, second * cosine + first * sine], axis=-1)


def pattern(queries, keys, values, pattern_dilation):
    length = queries.shape[0]
    unit = pattern_dilation * REACH_STEPS
    padded = -(-length // unit) * unit
    blocks = padded // unit

    def regroup(array):
        array = jnp.pad(array, ((0, padded - length), (0, 0), (0, 0)))
        return array.reshape(blocks, REACH_STEPS, pattern_dilation, HEADS, HEAD).astype(jnp.float32)

    def with_prev(array):
        earlier = jnp.pad(array, ((1, 0), (0, 0), (0, 0), (0, 0), (0, 0)))[:-1]
        return jnp.concatenate([earlier, array], axis=1)

    query_sub = regroup(queries)
    key_sub = with_prev(regroup(keys))
    value_sub = with_prev(regroup(values))
    scores = jnp.einsum('nqrhd,nkrhd->nrhqk', query_sub, key_sub) * HEAD ** -0.5
    query_index = jnp.arange(REACH_STEPS)[:, None] + REACH_STEPS
    key_index = jnp.arange(2 * REACH_STEPS)[None, :]
    distance = query_index - key_index
    key_global = jnp.arange(blocks)[:, None, None] * REACH_STEPS + key_index[None] - REACH_STEPS
    allowed = ((distance >= 0) & (distance <= REACH_STEPS))[None] & (key_global >= 0)
    scores = jnp.where(allowed[:, None, None], scores, -jnp.inf)
    top = jnp.max(scores, axis=-1, keepdims=True)
    offset_keys = jnp.exp(scores - top)
    total = jnp.sum(offset_keys, axis=-1, keepdims=True)
    weights = lax.optimization_barrier((offset_keys / total).astype(jnp.bfloat16)).astype(jnp.float32)
    result = jnp.einsum('nrhqk,nkrhd->nqrhd', weights, value_sub).reshape(padded, HEADS, HEAD)[:length]
    lse = jnp.transpose((top + jnp.log(total))[..., 0], (0, 3, 1, 2)).reshape(padded, HEADS)[:length]
    return result, lse


def reference(tokens, query_weight, key_weight, value_weight, output_weight):
    length = tokens.shape[0]
    positions = jnp.arange(length).astype(jnp.float32)
    query_proj = jnp.dot(tokens, query_weight, preferred_element_type=jnp.float32).reshape(length, HEADS, HEAD)
    key_proj = jnp.dot(tokens, key_weight, preferred_element_type=jnp.float32).reshape(length, HEADS, HEAD)
    queries = rotate(query_proj, positions).astype(jnp.bfloat16)
    keys = rotate(key_proj, positions).astype(jnp.bfloat16)
    values = jnp.dot(tokens, value_weight, preferred_element_type=jnp.float32).astype(jnp.bfloat16)
    values = values.reshape(length, HEADS, HEAD)
    results = []
    lses = []
    for pattern_dilation in (1, MIDDLE_DILATION, FAR_DILATION):
        result, lse = pattern(queries, keys, values, pattern_dilation)
        results.append(result)
        lses.append(lse)
    mixing = jax.nn.softmax(jnp.stack(lses, axis=0), axis=0)
    mixed = jnp.sum(mixing[..., None] * jnp.stack(results, axis=0), axis=0)
    mixed = mixed.astype(jnp.bfloat16).reshape(length, HEADS * HEAD)
    return jnp.dot(mixed, output_weight, preferred_element_type=jnp.float32).astype(jnp.bfloat16)
```

```python
import functools
import math

import jax
import jax.numpy as jnp
from jax import lax
from jax.experimental import pallas as pl
from jax.experimental.pallas import tpu as pltpu
from jax.sharding import PartitionSpec as P

HEAD = 128
REACH_STEPS = 128
MIDDLE_DILATION = 4
FAR_DILATION = 16
THETA_BASE = 500000.0

MESH = pl.DeviceIdType.MESH
F32 = jnp.float32
BF16 = jnp.bfloat16
G = MIDDLE_DILATION
T = REACH_STEPS
ROWS = G * T
NEG = -1e30
SCALE = HEAD**-0.5 * math.log2(math.e)
NT = (((1,), (1,)), ((), ()))


def iota(shape, dim):
    return lax.broadcasted_iota(jnp.int32, shape, dim)


def sin_cos(x):
    n = jnp.floor(x * (2.0 / math.pi) + 0.5)
    r = ((x - n * 1.5703125) - n * 4.837512969970703125e-4) - n * 7.549789954891882e-8
    z = r * r
    s = r + r * z * ((-1.9515295891e-4 * z + 8.3321608736e-3) * z - 1.6666654611e-1)
    c = 1.0 - 0.5 * z + z * z * ((2.443315711809948e-5 * z - 1.388731625493765e-3) * z + 4.166664568298827e-2)
    k = n.astype(jnp.int32) & 3
    odd = (k & 1) == 1
    sine = jnp.where(odd, c, s)
    cosine = jnp.where(odd, s, c)
    sine = jnp.where((k & 2) == 2, -sine, sine)
    cosine = jnp.where(((k + 1) & 2) == 2, -cosine, cosine)
    return sine, cosine


def kernel(n, tokens, wq, wk, wv, wo, out,
           x_nat, x, wq_v, wk_v, wv_v, wo_v, out_v,
           rope_c, rope_s, bias, bias2, bias3, perm_in, perm_out,
           q0, k0, v0, k1, v1, q1, q3,
           o3, l3, o3_in, l3_in, o1, l1, o1_in, l1_in,
           loc_o, loc_m, loc_l, mix_t, mixed,
           load_sem, tok_sem, k_sem, v_sem, q1_sem, q3_sem,
           o3_sem, l3_sem, o1_sem, l1_sem, mix_sem, out_sem):
    c = lax.axis_index("sp")
    tp = lax.axis_index("tp")
    heads = k0.shape[0]
    chunks = 2 * heads
    pairs = heads // 2
    half_rows = ROWS // 2

    def at(distance):
        return {"sp": lax.rem(c + distance + n, n)}

    partner = {"tp": 1 - tp}

    def load(i):
        src, dst = ((tokens, x_nat.at[tp]), (wk, wk_v), (wv, wv_v), (wq, wq_v), (wo, wo_v))[i]
        return pltpu.make_async_copy(src, dst, load_sem.at[i])

    for i in range(5):
        load(i).start()

    barrier = pltpu.get_barrier_semaphore()
    greeted = [partner, at(1), at(-1), at(2), at(-2)]
    for device in greeted:
        pl.semaphore_signal(barrier, inc=1, device_id=device, device_id_type=MESH)

    def remote(src, dst, sems, i, device):
        return pltpu.make_async_remote_copy(
            src_ref=src, dst_ref=dst, send_sem=sems.at[0, i], recv_sem=sems.at[1, i],
            device_id=device, device_id_type=MESH)

    def send_tokens():
        return remote(tokens, x_nat.at[tp], tok_sem, 0, partner)

    def send_k(h):
        return remote(k0.at[h], k1.at[h], k_sem, h, at(1))

    def send_v(h):
        return remote(v0.at[h], v1.at[h], v_sem, h, at(1))

    def chunk(ref, i):
        return ref.at[pl.ds(2 * i, 2)]

    def send_q1(i):
        return remote(chunk(q0, i), chunk(q1, i), q1_sem, i, at(-1))

    def send_q3(i):
        return remote(chunk(q1, i), chunk(q3, i), q3_sem, i, at(-2))

    def send_o3(i):
        return (remote(chunk(o3, i), chunk(o3_in, i), o3_sem, i, at(2)),
                remote(chunk(l3, i), chunk(l3_in, i), l3_sem, i, at(2)))

    def send_o1(i):
        return (remote(chunk(o1, i), chunk(o1_in, i), o1_sem, i, at(1)),
                remote(chunk(l1, i), chunk(l1_in, i), l1_sem, i, at(1)))

    def send_mixed(p):
        return remote(mixed.at[tp, p], mixed.at[tp, p], mix_sem, p, partner)

    def send_out(b):
        rows = pl.ds(b * T, T)
        return pltpu.make_async_copy(out_v.at[rows], out.at[rows], out_sem.at[b])

    pl.semaphore_wait(barrier, len(greeted))
    send_tokens().start()

    row = iota((half_rows, half_rows), 0)
    col = iota((half_rows, half_rows), 1)
    perm_in[...] = jnp.where(row == (col & (G - 1)) * (half_rows // G) + lax.shift_right_logical(col, 2), 1.0, 0.0).astype(BF16)

    lane = iota((T, HEAD), 1)
    index = lane & (HEAD // 2 - 1)
    inverse = jnp.ones((T, HEAD), F32)
    for bit in range(6):
        factor = THETA_BASE ** (-(2.0**bit) / (HEAD // 2))
        inverse = jnp.where((lax.shift_right_logical(index, bit) & 1) == 1, inverse * factor, inverse)

    @pl.loop(0, G)
    def _(g):
        position = c * ROWS + iota((T, HEAD), 0) * G + g
        sine, cosine = sin_cos(position.astype(F32) * inverse)
        rows = pl.ds(g * T, T)
        rope_c[rows, :] = cosine
        rope_s[rows, :] = jnp.where(lane < HEAD // 2, -sine, sine)

    load(0).wait()

    def permuted(u):
        half = T // 2
        y = jnp.dot(perm_in[...], x_nat[u], preferred_element_type=F32).astype(BF16)
        for g in range(G):
            x[pl.ds(g * T + u * half, half), :] = y[g * half:(g + 1) * half]

    permuted(tp)

    jk = iota((T, T), 0)
    jq = iota((T, T), 1)
    same = ((jq - jk) & (FAR_DILATION // MIDDLE_DILATION - 1)) == 0
    far = jnp.where(same, 0.0, NEG)
    bias2[...] = far + jnp.where((c + 1 < n) & (c >= 1), 0.0, NEG)
    bias3[0] = jnp.where(same & (jk >= jq), 0.0, NEG) + jnp.where((c + 3 < n) & (c >= 1), 0.0, NEG)
    bias3[1] = far + jnp.where(c + 3 < n, 0.0, NEG)

    send_tokens().wait_recv()
    permuted(1 - tp)

    def rotated(y):
        return (y * rope_c[...] + pltpu.roll(y, HEAD // 2, 1) * rope_s[...]).astype(BF16)

    load(1).wait()
    load(2).wait()
    load(3).wait()
    for p in range(pairs):
        cols = slice(2 * p * HEAD, (2 * p + 2) * HEAD)
        y = jnp.dot(x[...], wk_v[:, cols], preferred_element_type=F32)
        for s in range(2):
            k0[2 * p + s] = rotated(y[:, s * HEAD:(s + 1) * HEAD])
        y = jnp.dot(x[...], wv_v[:, cols], preferred_element_type=F32).astype(BF16)
        for s in range(2):
            v0[2 * p + s] = y[:, s * HEAD:(s + 1) * HEAD].T
            send_k(2 * p + s).start()
        y = jnp.dot(x[...], wq_v[:, cols], preferred_element_type=F32)
        for s in range(2):
            h = 2 * p + s
            send_v(h).start()
            z = rotated(y[:, s * HEAD:(s + 1) * HEAD])
            for g in range(G):
                q0[h * G + g] = z[g * T:(g + 1) * T]
        for i in range(4 * p, 4 * p + 4):
            send_q1(i).start()

    @pl.loop(0, 2 * G)
    def _(b):
        which = lax.shift_right_logical(b, 2)
        gk = b & (G - 1)

        @pl.loop(0, G)
        def _(gq):
            k_pos = (iota((T, T), 0) - T * (1 - which)) * G + gk
            d = iota((T, T), 1) * G + gq - k_pos
            ok = d >= 0
            near = jnp.where(ok & (d <= REACH_STEPS), 1, 0)
            mid = jnp.where(ok & (d <= REACH_STEPS * MIDDLE_DILATION) & ((d & (MIDDLE_DILATION - 1)) == 0), 1, 0)
            wide = jnp.where(ok & (d <= REACH_STEPS * FAR_DILATION) & ((d & (FAR_DILATION - 1)) == 0), 1, 0)
            count = near + mid + wide
            value = jnp.where(count == 3, math.log2(3.0), jnp.where(count == 2, 1.0, jnp.where(count == 1, 0.0, NEG)))
            value = value + jnp.where((which == 1) | (c >= 1), 0.0, NEG)
            bias[gq, which, pl.ds(gk * T, T), :] = value

    @pl.loop(0, G)
    def _(g):
        t = g * T + iota((T, ROWS), 0)
        s = iota((T, ROWS), 1)
        perm_out[pl.ds(g * T, T), :] = jnp.where(
            s == (t & (G - 1)) * T + lax.shift_right_logical(t, 2), 1.0, 0.0).astype(BF16)

    @pl.loop(0, chunks)
    def _(i):
        send_q1(i).wait_recv()
        send_q3(i).start()

    def softmax_of(scores):
        top = functools.reduce(jnp.maximum, [jnp.max(s, axis=0, keepdims=True) for s in scores])
        ps = [jnp.exp2(s - top) for s in scores]
        total = functools.reduce(jnp.add, [jnp.sum(p, axis=0, keepdims=True) for p in ps])
        return top, total, [p.astype(BF16) for p in ps]

    def scores_of(keys, queries, b):
        return lax.dot_general(keys, queries, NT, preferred_element_type=F32) * SCALE + b

    def tile(g):
        return pl.ds(pl.multiple_of(g * T, T), T)

    @pl.loop(0, heads)
    def _(h):
        send_k(h).wait_recv()
        send_v(h).wait_recv()

        @pl.loop(2 * h, 2 * h + 2)
        def _(i):
            send_q3(i).wait_recv()
            for s in range(2):
                t = 2 * i + s
                g = t - h * G
                q = q3[t]
                top, total, (p4, p3) = softmax_of([
                    scores_of(k1[h, tile(g), :], q, bias3[0]),
                    scores_of(k0[h, tile(g), :], q, bias3[1])])
                o = (jnp.dot(v1[h, :, tile(g)], p4, preferred_element_type=F32)
                     + jnp.dot(v0[h, :, tile(g)], p3, preferred_element_type=F32))
                o3[t] = (o * (1.0 / total)).astype(BF16)
                l3[t] = top + jnp.log2(total)
            for copy in send_o3(i):
                copy.start()

        @pl.loop(0, G)
        def _(g):
            q = q0[h * G + g]
            top, total, (p_prev, p_own) = softmax_of([
                scores_of(k1[h], q, bias[g, 0]), scores_of(k0[h], q, bias[g, 1])])
            o = (jnp.dot(v1[h], p_prev, preferred_element_type=F32)
                 + jnp.dot(v0[h], p_own, preferred_element_type=F32))
            loc_o[h * G + g] = o
            loc_m[h * G + g] = top
            loc_l[h * G + g] = total

    @pl.loop(0, chunks)
    def _(i):
        for copy in send_o3(i):
            copy.wait_recv()
        h = lax.div(i, 2)
        for s in range(2):
            t = 2 * i + s
            g = t - h * G
            top, total, (p2,) = softmax_of([scores_of(k1[h, tile(g), :], q1[t], bias2[...])])
            o = jnp.dot(v1[h, :, tile(g)], p2, preferred_element_type=F32)
            lse = l3_in[t]
            peak = jnp.maximum(top, lse)
            here = jnp.exp2(top - peak)
            there = jnp.exp2(lse - peak)
            whole = total * here + there
            o1[t] = (o * (here / whole) + o3_in[t].astype(F32) * (there / whole)).astype(BF16)
            l1[t] = peak + jnp.log2(whole)
        for copy in send_o1(i):
            copy.start()

    for p in range(pairs):
        for s in range(2):
            h = 2 * p + s
            for i in (2 * h, 2 * h + 1):
                for copy in send_o1(i):
                    copy.wait_recv()
                for t in (2 * i, 2 * i + 1):
                    top, lse = loc_m[t], l1_in[t]
                    peak = jnp.maximum(top, lse)
                    here = jnp.exp2(top - peak)
                    there = jnp.exp2(lse - peak)
                    whole = loc_l[t] * here + there
                    o = loc_o[t] * (here / whole) + o1_in[t].astype(F32) * (there / whole)
                    mix_t[h, :, (t - h * G) * T:(t - h * G + 1) * T] = o.astype(BF16)
            mixed[tp, p, :, s * HEAD:(s + 1) * HEAD] = lax.dot_general(
                perm_out[...], mix_t[h], NT, preferred_element_type=F32).astype(BF16)
        send_mixed(p).start()

    load(4).wait()
    for p in range(pairs):
        send_mixed(p).wait_recv()
    width = 2 * HEAD
    for b in range(G):
        rows = pl.ds(b * T, T)
        total = None
        for u in range(2):
            for p in range(pairs):
                start = (u * pairs + p) * width
                term = jnp.dot(mixed[u, p, rows, :], wo_v[start:start + width, :], preferred_element_type=F32)
                total = term if total is None else total + term
        out_v[rows, :] = total.astype(BF16)
        send_out(b).start()

    send_tokens().wait_send()
    for h in range(heads):
        send_k(h).wait_send()
        send_v(h).wait_send()

    @pl.loop(0, chunks)
    def _(i):
        for copy in (send_q1(i), send_q3(i), *send_o3(i), *send_o1(i)):
            copy.wait_send()

    for p in range(pairs):
        send_mixed(p).wait_send()
    for b in range(G):
        send_out(b).wait()


def body(tokens, query_weight, key_weight, value_weight, output_weight):
    n = lax.axis_size("sp")
    half_rows, depth = tokens.shape
    width = query_weight.shape[1]
    heads = width // HEAD
    tiles, chunks, pairs = heads * G, 2 * heads, heads // 2
    features = output_weight.shape[1]
    assert 2 * half_rows == ROWS and FAR_DILATION == MIDDLE_DILATION**2 and heads % 2 == 0
    assert output_weight.shape[0] == 2 * width
    vmem = pltpu.VMEM
    dma = pltpu.SemaphoreType.DMA
    square = (tiles, T, HEAD)
    stat = (tiles, 1, T)
    scratch = [
        vmem((2, half_rows, depth), BF16), vmem((ROWS, depth), BF16),
        vmem((depth, width), BF16), vmem((depth, width), BF16), vmem((depth, width), BF16),
        vmem((2 * width, features), BF16), vmem((ROWS, features), BF16),
        vmem((ROWS, HEAD), F32), vmem((ROWS, HEAD), F32),
        vmem((G, 2, ROWS, T), F32), vmem((T, T), F32), vmem((2, T, T), F32),
        vmem((half_rows, half_rows), BF16), vmem((ROWS, ROWS), BF16),
        vmem(square, BF16),
        vmem((heads, ROWS, HEAD), BF16), vmem((heads, HEAD, ROWS), BF16),
        vmem((heads, ROWS, HEAD), BF16), vmem((heads, HEAD, ROWS), BF16),
        vmem(square, BF16), vmem(square, BF16),
        vmem(square, BF16), vmem(stat, F32), vmem(square, BF16), vmem(stat, F32),
        vmem(square, BF16), vmem(stat, F32), vmem(square, BF16), vmem(stat, F32),
        vmem(square, F32), vmem(stat, F32), vmem(stat, F32),
        vmem((heads, HEAD, ROWS), BF16), vmem((2, pairs, ROWS, 2 * HEAD), BF16),
        dma((5,)), dma((2, 1)), dma((2, heads)), dma((2, heads)), dma((2, chunks)), dma((2, chunks)),
        dma((2, chunks)), dma((2, chunks)), dma((2, chunks)), dma((2, chunks)), dma((2, pairs)), dma((G,)),
    ]
    hbm = pl.BlockSpec(memory_space=pl.ANY)
    return pl.pallas_call(
        functools.partial(kernel, n),
        out_shape=jax.ShapeDtypeStruct((ROWS, features), BF16),
        in_specs=[hbm] * 5,
        out_specs=hbm,
        scratch_shapes=scratch,
        compiler_params=pltpu.CompilerParams(
            collective_id=0, has_side_effects=True, vmem_limit_bytes=60 * 1024 * 1024),
        name="attention",
    )(tokens, query_weight, key_weight, value_weight, output_weight)


def solution(mesh):
    in_specs = (
        P(("grp", "sp", "tp"), None),
        P(None, "tp"),
        P(None, "tp"),
        P(None, "tp"),
        P(None, "tp"),
    )
    out_specs = P(("grp", "sp"), "tp")
    return jax.shard_map(body, mesh=mesh, in_specs=in_specs, out_specs=out_specs, check_vma=False)
```

```python
import functools
import math

import jax
import jax.numpy as jnp
from jax import lax
from jax.experimental import pallas as pl
from jax.experimental.pallas import tpu as pltpu
from jax.sharding import PartitionSpec as P

HEAD = 128
REACH_STEPS = 128
MIDDLE_DILATION = 4
FAR_DILATION = 16
THETA_BASE = 500000.0

MESH = pl.DeviceIdType.MESH
F32 = jnp.float32
BF16 = jnp.bfloat16
G = MIDDLE_DILATION
T = REACH_STEPS
ROWS = G * T
NEG = -1e30
VMEM_LIMIT = 64000000
SCALE = HEAD**-0.5 * math.log2(math.e)
NT = (((1,), (1,)), ((), ()))


def iota(shape, dim):
    return lax.broadcasted_iota(jnp.int32, shape, dim)


def sin_cos(x):
    n = jnp.floor(x * (2.0 / math.pi) + 0.5)
    r = ((x - n * 1.5703125) - n * 4.837512969970703125e-4) - n * 7.549789954891882e-8
    z = r * r
    s = r + r * z * ((-1.9515295891e-4 * z + 8.3321608736e-3) * z - 1.6666654611e-1)
    c = 1.0 - 0.5 * z + z * z * ((2.443315711809948e-5 * z - 1.388731625493765e-3) * z + 4.166664568298827e-2)
    k = n.astype(jnp.int32) & 3
    odd = (k & 1) == 1
    sine = jnp.where(odd, c, s)
    cosine = jnp.where(odd, s, c)
    sine = jnp.where((k & 2) == 2, -sine, sine)
    cosine = jnp.where(((k + 1) & 2) == 2, -cosine, cosine)
    return sine, cosine


def kernel(n, tokens, wq, wk, wv, wo, out,
           x_nat, x, wq_v, wk_v, wv_v, wo_v, out_v, acc,
           rope_c, rope_s, bias, bias2, bias3, perm_in, perm_out,
           q0, k0, v0, k1, v1, v0t, v1t, q1, q3,
           o3, l3, o3_in, l3_in, o1, l1, o1_in, l1_in,
           loc_o, loc_m, loc_l, mix_t, mixed,
           load_sem, tok_sem, k_sem, v_sem, q1_sem, q3_sem,
           o3_sem, l3_sem, o1_sem, l1_sem, mix_sem, out_sem):
    c = lax.axis_index("sp")
    tp = lax.axis_index("tp")
    heads = k0.shape[0]
    width = heads * HEAD
    chunks = 2 * heads
    pairs = heads // 2
    half_rows = ROWS // 2
    piece = T // 2
    partner = {"tp": 1 - tp}

    before = [None, c >= 1, c >= 2]
    after = [None, c + 1 < n, c + 2 < n, c + 3 < n]

    def at(distance):
        return {"sp": jnp.clip(c + distance, 0, n - 1)}

    def load(i):
        src, dst = ((tokens, x_nat.at[tp]), (wk, wk_v), (wv, wv_v), (wq, wq_v), (wo, wo_v))[i]
        return pltpu.make_async_copy(src, dst, load_sem.at[i])

    for i in range(5):
        load(i).start()

    barrier = pltpu.get_barrier_semaphore()

    def greet(device):
        pl.semaphore_signal(barrier, inc=1, device_id=device, device_id_type=MESH)

    greet(partner)
    for distance in (1, 2):
        pl.when(after[distance])(functools.partial(greet, at(distance)))
        pl.when(before[distance])(functools.partial(greet, at(-distance)))

    def remote(src, dst, sems, i, device):
        return pltpu.make_async_remote_copy(
            src_ref=src, dst_ref=dst, send_sem=sems.at[0, i], recv_sem=sems.at[1, i],
            device_id=device, device_id_type=MESH)

    def send_tokens():
        return remote(tokens, x_nat.at[tp], tok_sem, 0, partner)

    def send_k(h, u):
        return remote(k0.at[h, :, u], k1.at[h, :, u], k_sem, 2 * h + u, at(1))

    def send_v(h, u):
        return remote(v0.at[h, :, u], v1.at[h, :, u], v_sem, 2 * h + u, at(1))

    def chunk(ref, i):
        return ref.at[pl.ds(2 * i, 2)]

    def send_q1(i):
        return remote(chunk(q0, i), chunk(q1, i), q1_sem, i, at(-1))

    def send_q3(i):
        return remote(chunk(q1, i), chunk(q3, i), q3_sem, i, at(-2))

    def send_o3(i):
        return (remote(chunk(o3, i), chunk(o3_in, i), o3_sem, i, at(2)),
                remote(chunk(l3, i), chunk(l3_in, i), l3_sem, i, at(2)))

    def send_o1(i):
        return (remote(chunk(o1, i), chunk(o1_in, i), o1_sem, i, at(1)),
                remote(chunk(l1, i), chunk(l1_in, i), l1_sem, i, at(1)))

    def send_mixed(h):
        return remote(mixed.at[tp, h], mixed.at[tp, h], mix_sem, h, partner)

    def send_out(b):
        rows = pl.ds(b * T, T)
        return pltpu.make_async_copy(out_v.at[rows], out.at[rows], out_sem.at[b])

    with jax.named_scope("tables"):
        row = iota((half_rows, half_rows), 0)
        col = iota((half_rows, half_rows), 1)
        perm_in[...] = jnp.where(row == (col & (G - 1)) * piece + lax.shift_right_logical(col, 2), 1.0, 0.0).astype(BF16)

        lane = iota((T, HEAD), 1)
        index = lane & (HEAD // 2 - 1)
        inverse = jnp.ones((T, HEAD), F32)
        for bit in range(6):
            factor = THETA_BASE ** (-(2.0**bit) / (HEAD // 2))
            inverse = jnp.where((lax.shift_right_logical(index, bit) & 1) == 1, inverse * factor, inverse)

        @pl.loop(0, 4)
        def _(i):
            u = lax.shift_right_logical(i, 1)
            r = iota((T, HEAD), 0) + (i & 1) * T
            local = (r & (piece - 1)) * G + lax.shift_right_logical(r, 6)
            position = c * ROWS + u * half_rows + local
            sine, cosine = sin_cos(position.astype(F32) * inverse)
            rows = pl.ds(pl.multiple_of((i & 1) * T, T), T)
            rope_c[u, rows, :] = cosine
            rope_s[u, rows, :] = jnp.where(lane < HEAD // 2, -sine, sine)

    def permuted(u):
        x[u] = jnp.dot(perm_in[...], x_nat[u], preferred_element_type=F32).astype(BF16)

    def columns(p):
        return slice(2 * p * HEAD, (2 * p + 2) * HEAD)

    def rotated(y, u):
        return (y * rope_c[u] + pltpu.roll(y, HEAD // 2, 1) * rope_s[u]).astype(BF16)

    def project(w, p, u):
        return jnp.dot(x[u], w[:, columns(p)], preferred_element_type=F32)

    def make_k(p, u):
        y = project(wk_v, p, u)
        for s in range(2):
            z = rotated(y[:, s * HEAD:(s + 1) * HEAD], u)
            for g in range(G):
                k0[2 * p + s, g, u] = z[g * piece:(g + 1) * piece]

    def make_v(p, u):
        y = project(wv_v, p, u).astype(BF16)
        for s in range(2):
            for g in range(G):
                v0[2 * p + s, g, u] = y[g * piece:(g + 1) * piece, s * HEAD:(s + 1) * HEAD]

    def forward(send, p, u):
        @pl.when(after[1])
        def _():
            for s in range(2):
                send(2 * p + s, u).start()

    with jax.named_scope("own_k"):
        load(0).wait()
        permuted(tp)
        load(1).wait()
        make_k(0, tp)

    with jax.named_scope("barrier"):
        count = 1
        for exists in (before[1], before[2], after[1], after[2]):
            count = count + exists.astype(jnp.int32)
        pl.semaphore_wait(barrier, count)
        send_tokens().start()

    with jax.named_scope("own_kv"):
        forward(send_k, 0, tp)
        load(2).wait()
        make_v(0, tp)
        forward(send_v, 0, tp)
        make_k(1, tp)
        forward(send_k, 1, tp)
        make_v(1, tp)
        forward(send_v, 1, tp)

    @pl.when(c < 1)
    def _():
        k1[...] = jnp.zeros_like(k1)
        v1[...] = jnp.zeros_like(v1)

    @pl.when(c < 2)
    def _():
        o3_in[...] = jnp.zeros_like(o3_in)
        l3_in[...] = jnp.full_like(l3_in, NEG)
        o1_in[...] = jnp.zeros_like(o1_in)
        l1_in[...] = jnp.full_like(l1_in, NEG)

    with jax.named_scope("tokwait"):
        send_tokens().wait_recv()

    with jax.named_scope("other_kv"):
        permuted(1 - tp)
        for p in range(pairs):
            make_k(p, 1 - tp)
            forward(send_k, p, 1 - tp)
            make_v(p, 1 - tp)
            forward(send_v, p, 1 - tp)

    with jax.named_scope("q"):
        load(3).wait()
        for p in range(pairs):
            y = jnp.dot(x[...].reshape(ROWS, x.shape[2]), wq_v[:, columns(p)], preferred_element_type=F32)
            for s in range(2):
                for u in range(2):
                    z = rotated(y[u * half_rows:(u + 1) * half_rows, s * HEAD:(s + 1) * HEAD], u)
                    for g in range(G):
                        q0[(2 * p + s) * G + g, u] = z[g * piece:(g + 1) * piece]
            if p == 0:
                @pl.when(before[2])
                def _():
                    for i in range(chunks // 2):
                        send_q1(i).start()

    with jax.named_scope("bias"):
        jk = iota((T, T), 0)
        jq = iota((T, T), 1)
        same = ((jq - jk) & (FAR_DILATION // MIDDLE_DILATION - 1)) == 0
        far = jnp.where(same, 0.0, NEG)
        bias2[...] = far
        bias3[0] = jnp.where(same & (jk >= jq), 0.0, NEG) + jnp.where(before[1], 0.0, NEG)
        bias3[1] = far

        @pl.loop(0, 2 * G)
        def _(b):
            which = lax.shift_right_logical(b, 2)
            gk = b & (G - 1)

            @pl.loop(0, G)
            def _(gq):
                k_pos = (iota((T, T), 0) - T * (1 - which)) * G + gk
                d = iota((T, T), 1) * G + gq - k_pos
                ok = d >= 0
                near = jnp.where(ok & (d <= REACH_STEPS), 1, 0)
                mid = jnp.where(ok & (d <= REACH_STEPS * MIDDLE_DILATION) & ((d & (MIDDLE_DILATION - 1)) == 0), 1, 0)
                wide = jnp.where(ok & (d <= REACH_STEPS * FAR_DILATION) & ((d & (FAR_DILATION - 1)) == 0), 1, 0)
                times = near + mid + wide
                value = jnp.where(times == 3, math.log2(3.0), jnp.where(times == 2, 1.0, jnp.where(times == 1, 0.0, NEG)))
                value = value + jnp.where((which == 1) | before[1], 0.0, NEG)
                bias[gq, which, pl.ds(pl.multiple_of(gk * T, T), T), :] = value

    with jax.named_scope("fwdq"):
        def pass_on(i):
            @pl.when(before[1] & after[1])
            def _():
                send_q1(i).wait_recv()

                @pl.when(before[2])
                def _():
                    send_q3(i).start()

        @pl.loop(0, chunks // 2)
        def _(i):
            pass_on(i)

            @pl.when(before[2])
            def _():
                send_q1(chunks // 2 + i).start()

        @pl.loop(0, G)
        def _(g):
            t = g * T + iota((T, ROWS), 0)
            s = iota((T, ROWS), 1)
            perm_out[pl.ds(pl.multiple_of(g * T, T), T), :] = jnp.where(
                s == (t & (G - 1)) * T + lax.shift_right_logical(t, 2), 1.0, 0.0).astype(BF16)

        for h in range(heads):
            v0t[h] = v0[h].reshape(ROWS, HEAD).T

        @pl.loop(chunks // 2, chunks)
        def _(i):
            pass_on(i)

    def softmax_of(scores):
        top = functools.reduce(jnp.maximum, [jnp.max(s, axis=0, keepdims=True) for s in scores])
        ps = [jnp.exp2(s - top) for s in scores]
        total = functools.reduce(jnp.add, [jnp.sum(p, axis=0, keepdims=True) for p in ps])
        return top, total, [p.astype(BF16) for p in ps]

    def scores_of(keys, queries, b):
        return lax.dot_general(keys, queries, NT, preferred_element_type=F32) * SCALE + b

    def tile(g):
        return pl.ds(pl.multiple_of(g * T, T), T)

    def rows_of(ref, *where):
        return ref[where].reshape(-1, HEAD)

    with jax.named_scope("o3local"):
        @pl.loop(0, heads)
        def _(h):
            @pl.when(before[1])
            def _():
                for u in range(2):
                    send_k(h, u).wait_recv()
                    send_v(h, u).wait_recv()

            v1t[h] = rows_of(v1, h).T

            @pl.when(after[3])
            def _():
                @pl.loop(2 * h, 2 * h + 2)
                def _(i):
                    send_q3(i).wait_recv()
                    for s in range(2):
                        t = 2 * i + s
                        g = t - h * G
                        q = rows_of(q3, t)
                        top, total, (p4, p3) = softmax_of([
                            scores_of(rows_of(k1, h, g), q, bias3[0]),
                            scores_of(rows_of(k0, h, g), q, bias3[1])])
                        o = (jnp.dot(v1t[h, :, tile(g)], p4, preferred_element_type=F32)
                             + jnp.dot(v0t[h, :, tile(g)], p3, preferred_element_type=F32))
                        o3[t] = (o * (1.0 / total)).astype(BF16)
                        l3[t] = top + jnp.log2(total)
                    for copy in send_o3(i):
                        copy.start()

            @pl.loop(0, G)
            def _(g):
                q = rows_of(q0, h * G + g)
                top, total, (p_prev, p_own) = softmax_of([
                    scores_of(rows_of(k1, h), q, bias[g, 0]), scores_of(rows_of(k0, h), q, bias[g, 1])])
                o = (jnp.dot(v1t[h], p_prev, preferred_element_type=F32)
                     + jnp.dot(v0t[h], p_own, preferred_element_type=F32))
                loc_o[h * G + g] = o
                loc_m[h * G + g] = top
                loc_l[h * G + g] = total

    with jax.named_scope("o1"):
        @pl.when(before[1] & after[1])
        def _():
            @pl.loop(0, chunks)
            def _(i):
                @pl.when(before[2])
                def _():
                    for copy in send_o3(i):
                        copy.wait_recv()

                h = lax.div(i, 2)
                for s in range(2):
                    t = 2 * i + s
                    g = t - h * G
                    top, total, (p2,) = softmax_of([scores_of(rows_of(k1, h, g), rows_of(q1, t), bias2[...])])
                    o = jnp.dot(v1t[h, :, tile(g)], p2, preferred_element_type=F32)
                    lse = l3_in[t]
                    peak = jnp.maximum(top, lse)
                    here = jnp.exp2(top - peak)
                    there = jnp.exp2(lse - peak)
                    whole = total * here + there
                    o1[t] = (o * (here / whole) + o3_in[t].astype(F32) * (there / whole)).astype(BF16)
                    l1[t] = peak + jnp.log2(whole)
                for copy in send_o1(i):
                    copy.start()

    def row_block(b):
        return slice(b * T, (b + 1) * T)

    def term(u, h, b):
        start = pl.multiple_of(u * width + h * HEAD, HEAD)
        return jnp.dot(mixed[u, h, row_block(b), :], wo_v[pl.ds(start, HEAD), :], preferred_element_type=F32)

    with jax.named_scope("final"):
        load(4).wait()
        for h in range(heads):
            with jax.named_scope(f"head{h}"):
                @pl.when(before[2])
                def _():
                    for i in (2 * h, 2 * h + 1):
                        for copy in send_o1(i):
                            copy.wait_recv()

                for g in range(G):
                    t = h * G + g
                    top, lse = loc_m[t], l1_in[t]
                    peak = jnp.maximum(top, lse)
                    here = jnp.exp2(top - peak)
                    there = jnp.exp2(lse - peak)
                    whole = loc_l[t] * here + there
                    o = loc_o[t] * (here / whole) + o1_in[t].astype(F32) * (there / whole)
                    mix_t[h, :, g * T:(g + 1) * T] = o.astype(BF16)
                mixed[tp, h] = lax.dot_general(perm_out[...], mix_t[h], NT, preferred_element_type=F32).astype(BF16)
                send_mixed(h).start()
            with jax.named_scope(f"acc{h}"):
                for b in range(G):
                    y = term(tp, h, b)
                    acc[row_block(b)] = y if h == 0 else acc[row_block(b)] + y
                if h > 0:
                    send_mixed(h - 1).wait_recv()
                    for b in range(G):
                        acc[row_block(b)] += term(1 - tp, h - 1, b)

    with jax.named_scope("out"):
        send_mixed(heads - 1).wait_recv()
        for b in range(G):
            out_v[row_block(b)] = (acc[row_block(b)] + term(1 - tp, heads - 1, b)).astype(BF16)
            send_out(b).start()

    with jax.named_scope("drain"):
        send_tokens().wait_send()

        @pl.when(after[1])
        def _():
            for h in range(heads):
                for u in range(2):
                    send_k(h, u).wait_send()
                    send_v(h, u).wait_send()

        @pl.loop(0, chunks)
        def _(i):
            @pl.when(before[2])
            def _():
                send_q1(i).wait_send()

            @pl.when(before[2] & after[1])
            def _():
                send_q3(i).wait_send()

            @pl.when(after[3])
            def _():
                for copy in send_o3(i):
                    copy.wait_send()

            @pl.when(before[1] & after[1])
            def _():
                for copy in send_o1(i):
                    copy.wait_send()

        for h in range(heads):
            send_mixed(h).wait_send()
        for b in range(G):
            send_out(b).wait()


def body(tokens, query_weight, key_weight, value_weight, output_weight):
    n = lax.axis_size("sp")
    half_rows, depth = tokens.shape
    width = query_weight.shape[1]
    heads = width // HEAD
    tiles, chunks = heads * G, 2 * heads
    features = output_weight.shape[1]
    assert 2 * half_rows == ROWS and FAR_DILATION == MIDDLE_DILATION**2 and heads % 2 == 0
    assert output_weight.shape[0] == 2 * width
    vmem = pltpu.VMEM
    dma = pltpu.SemaphoreType.DMA
    split = (tiles, 2, T // 2, HEAD)
    by_head = (heads, G, 2, T // 2, HEAD)
    turned = (heads, HEAD, ROWS)
    square = (tiles, T, HEAD)
    stat = (tiles, 1, T)
    scratch = [
        vmem((2, half_rows, depth), BF16), vmem((2, half_rows, depth), BF16),
        vmem((depth, width), BF16), vmem((depth, width), BF16), vmem((depth, width), BF16),
        vmem((2 * width, features), BF16), vmem((ROWS, features), BF16), vmem((ROWS, features), F32),
        vmem((2, half_rows, HEAD), F32), vmem((2, half_rows, HEAD), F32),
        vmem((G, 2, ROWS, T), F32), vmem((T, T), F32), vmem((2, T, T), F32),
        vmem((half_rows, half_rows), BF16), vmem((ROWS, ROWS), BF16),
        vmem(split, BF16),
        vmem(by_head, BF16), vmem(by_head, BF16), vmem(by_head, BF16), vmem(by_head, BF16),
        vmem(turned, BF16), vmem(turned, BF16),
        vmem(split, BF16), vmem(split, BF16),
        vmem(square, BF16), vmem(stat, F32), vmem(square, BF16), vmem(stat, F32),
        vmem(square, BF16), vmem(stat, F32), vmem(square, BF16), vmem(stat, F32),
        vmem(square, F32), vmem(stat, F32), vmem(stat, F32),
        vmem(turned, BF16), vmem((2, heads, ROWS, HEAD), BF16),
        dma((5,)), dma((2, 1)), dma((2, chunks)), dma((2, chunks)), dma((2, chunks)), dma((2, chunks)),
        dma((2, chunks)), dma((2, chunks)), dma((2, chunks)), dma((2, chunks)), dma((2, heads)), dma((G,)),
    ]
    hbm = pl.BlockSpec(memory_space=pltpu.HBM)
    return pl.pallas_call(
        functools.partial(kernel, n),
        out_shape=jax.ShapeDtypeStruct((ROWS, features), BF16),
        in_specs=[hbm] * 5,
        out_specs=pl.BlockSpec(memory_space=pl.ANY),
        scratch_shapes=scratch,
        compiler_params=pltpu.CompilerParams(
            collective_id=0, has_side_effects=True, vmem_limit_bytes=VMEM_LIMIT),
        name="attention",
    )(tokens, query_weight, key_weight, value_weight, output_weight)


def solution(mesh):
    in_specs = (
        P(("grp", "sp", "tp"), None),
        P(None, "tp"),
        P(None, "tp"),
        P(None, "tp"),
        P(None, "tp"),
    )
    out_specs = P(("grp", "sp"), "tp")
    return jax.shard_map(body, mesh=mesh, in_specs=in_specs, out_specs=out_specs, check_vma=False)
```

```python
import functools
import math

import jax
import jax.numpy as jnp
from jax import lax
from jax.experimental import pallas as pl
from jax.experimental.pallas import tpu as pltpu
from jax.sharding import PartitionSpec as P

HEAD = 128
REACH_STEPS = 128
MIDDLE_DILATION = 4
FAR_DILATION = 16
THETA_BASE = 500000.0

MESH = pl.DeviceIdType.MESH
F32 = jnp.float32
BF16 = jnp.bfloat16
G = MIDDLE_DILATION
T = REACH_STEPS
ROWS = G * T
NEG = -1e30
VMEM_LIMIT = 55_000_000
SCALE = HEAD**-0.5 * math.log2(math.e)
NT = (((1,), (1,)), ((), ()))


def iota(shape, dim):
    return lax.broadcasted_iota(jnp.int32, shape, dim)


def sin_cos(x):
    n = jnp.floor(x * (2.0 / math.pi) + 0.5)
    r = ((x - n * 1.5703125) - n * 4.837512969970703125e-4) - n * 7.549789954891882e-8
    z = r * r
    s = r + r * z * ((-1.9515295891e-4 * z + 8.3321608736e-3) * z - 1.6666654611e-1)
    c = 1.0 - 0.5 * z + z * z * ((2.443315711809948e-5 * z - 1.388731625493765e-3) * z + 4.166664568298827e-2)
    k = n.astype(jnp.int32) & 3
    odd = (k & 1) == 1
    sine = jnp.where(odd, c, s)
    cosine = jnp.where(odd, s, c)
    sine = jnp.where((k & 2) == 2, -sine, sine)
    cosine = jnp.where(((k + 1) & 2) == 2, -cosine, cosine)
    return sine, cosine


def kernel(n, tokens, wq, wk, wv, wo, out,
           x_nat, x, wq_v, wk_v, wv_v, wo_v, out_v, acc,
           rope_c, rope_s, bias, bias2, bias3, perm_in, perm_out,
           q0, k0, v0, k1, v1, v0t, v1t, q1, q3,
           o3, l3, o3_in, l3_in, o1, l1, o1_in, l1_in,
           loc_o, loc_m, loc_l, mix_t, mixed,
           load_sem, tok_sem, k_sem, v_sem, q1_sem, q3_sem,
           o3_sem, l3_sem, o1_sem, l1_sem, mix_sem, out_sem):
    c = lax.axis_index("sp")
    tp = lax.axis_index("tp")
    heads = k0.shape[0]
    width = heads * HEAD
    chunks = 2 * heads
    pairs = heads // 2
    half_rows = ROWS // 2
    piece = T // 2
    partner = {"tp": 1 - tp}

    before = [None, c >= 1, c >= 2]
    after = [None, c + 1 < n, c + 2 < n, c + 3 < n]

    def at(distance):
        return {"sp": jnp.clip(c + distance, 0, n - 1)}

    def load(i):
        src, dst = ((tokens, x_nat.at[tp]), (wk, wk_v), (wv, wv_v), (wq, wq_v), (wo, wo_v))[i]
        return pltpu.make_async_copy(src, dst, load_sem.at[i])

    for i in range(5):
        load(i).start()

    barrier = pltpu.get_barrier_semaphore()

    def greet(device):
        pl.semaphore_signal(barrier, inc=1, device_id=device, device_id_type=MESH)

    greet(partner)
    for distance in (1, 2):
        pl.when(after[distance])(functools.partial(greet, at(distance)))
        pl.when(before[distance])(functools.partial(greet, at(-distance)))

    def remote(src, dst, sems, i, device):
        return pltpu.make_async_remote_copy(
            src_ref=src, dst_ref=dst, send_sem=sems.at[0, i], recv_sem=sems.at[1, i],
            device_id=device, device_id_type=MESH)

    def send_tokens():
        return remote(tokens, x_nat.at[tp], tok_sem, 0, partner)

    def send_k(h, u):
        return remote(k0.at[h, :, u], k1.at[h, :, u], k_sem, 2 * h + u, at(1))

    def send_v(h, u):
        return remote(v0.at[h, :, u], v1.at[h, :, u], v_sem, 2 * h + u, at(1))

    def chunk(ref, i):
        return ref.at[pl.ds(2 * i, 2)]

    def send_q1(i):
        return remote(chunk(q0, i), chunk(q1, i), q1_sem, i, at(-1))

    def send_q3(i):
        return remote(chunk(q1, i), chunk(q3, i), q3_sem, i, at(-2))

    def send_o3(i):
        return (remote(chunk(o3, i), chunk(o3_in, i), o3_sem, i, at(2)),
                remote(chunk(l3, i), chunk(l3_in, i), l3_sem, i, at(2)))

    def send_o1(i):
        return (remote(chunk(o1, i), chunk(o1_in, i), o1_sem, i, at(1)),
                remote(chunk(l1, i), chunk(l1_in, i), l1_sem, i, at(1)))

    def send_mixed(h):
        return remote(mixed.at[tp, h], mixed.at[tp, h], mix_sem, h, partner)

    def send_out(b):
        rows = pl.ds(b * T, T)
        return pltpu.make_async_copy(out_v.at[rows], out.at[rows], out_sem.at[b])

    with jax.named_scope("tables"):
        row = iota((half_rows, half_rows), 0)
        col = iota((half_rows, half_rows), 1)
        perm_in[...] = jnp.where(row == (col & (G - 1)) * piece + lax.shift_right_logical(col, 2), 1.0, 0.0).astype(BF16)

        lane = iota((T, HEAD), 1)
        index = lane & (HEAD // 2 - 1)
        inverse = jnp.ones((T, HEAD), F32)
        for bit in range(6):
            factor = THETA_BASE ** (-(2.0**bit) / (HEAD // 2))
            inverse = jnp.where((lax.shift_right_logical(index, bit) & 1) == 1, inverse * factor, inverse)

        @pl.loop(0, 4)
        def _(i):
            u = lax.shift_right_logical(i, 1)
            r = iota((T, HEAD), 0) + (i & 1) * T
            local = (r & (piece - 1)) * G + lax.shift_right_logical(r, 6)
            position = c * ROWS + u * half_rows + local
            sine, cosine = sin_cos(position.astype(F32) * inverse)
            rows = pl.ds(pl.multiple_of((i & 1) * T, T), T)
            rope_c[u, rows, :] = cosine
            rope_s[u, rows, :] = jnp.where(lane < HEAD // 2, -sine, sine)

    def permuted(u):
        x[u] = jnp.dot(perm_in[...], x_nat[u], preferred_element_type=F32).astype(BF16)

    def columns(p):
        return slice(2 * p * HEAD, (2 * p + 2) * HEAD)

    def rotated(y, u):
        return (y * rope_c[u] + pltpu.roll(y, HEAD // 2, 1) * rope_s[u]).astype(BF16)

    def project(w, p, u):
        return jnp.dot(x[u], w[:, columns(p)], preferred_element_type=F32)

    def make_k(p, u):
        y = project(wk_v, p, u)
        for s in range(2):
            z = rotated(y[:, s * HEAD:(s + 1) * HEAD], u)
            for g in range(G):
                k0[2 * p + s, g, u] = z[g * piece:(g + 1) * piece]

    def make_v(p, u):
        y = project(wv_v, p, u).astype(BF16)
        for s in range(2):
            for g in range(G):
                v0[2 * p + s, g, u] = y[g * piece:(g + 1) * piece, s * HEAD:(s + 1) * HEAD]

    def forward(send, p, u):
        @pl.when(after[1])
        def _():
            for s in range(2):
                send(2 * p + s, u).start()

    with jax.named_scope("own_k"):
        load(0).wait()
        permuted(tp)
        load(1).wait()
        make_k(0, tp)

    with jax.named_scope("barrier"):
        count = 1
        for exists in (before[1], before[2], after[1], after[2]):
            count = count + exists.astype(jnp.int32)
        pl.semaphore_wait(barrier, count)
        send_tokens().start()

    with jax.named_scope("own_kv"):
        forward(send_k, 0, tp)
        load(2).wait()
        make_v(0, tp)
        forward(send_v, 0, tp)

    @pl.when(c < 1)
    def _():
        k1[...] = jnp.zeros_like(k1)
        v1[...] = jnp.zeros_like(v1)

    @pl.when(c < 2)
    def _():
        o3_in[...] = jnp.zeros_like(o3_in)
        l3_in[...] = jnp.full_like(l3_in, NEG)
        o1_in[...] = jnp.zeros_like(o1_in)
        l1_in[...] = jnp.full_like(l1_in, NEG)

    def make_q(p):
        y = jnp.dot(x[...].reshape(ROWS, x.shape[2]), wq_v[:, columns(p)], preferred_element_type=F32)
        for s in range(2):
            for u in range(2):
                z = rotated(y[u * half_rows:(u + 1) * half_rows, s * HEAD:(s + 1) * HEAD], u)
                for g in range(G):
                    q0[(2 * p + s) * G + g, u] = z[g * piece:(g + 1) * piece]

    half = chunks // 2

    def ask(p):
        @pl.when(before[2])
        def _():
            for i in range(p * half, (p + 1) * half):
                send_q1(i).start()

    with jax.named_scope("own_kv1"):
        make_k(1, tp)

    with jax.named_scope("tokwait"):
        send_tokens().wait_recv()

    with jax.named_scope("other_kv0"):
        permuted(1 - tp)
        make_k(0, 1 - tp)
        forward(send_k, 0, 1 - tp)
        make_v(0, 1 - tp)
        forward(send_v, 0, 1 - tp)
        forward(send_k, 1, tp)

    with jax.named_scope("q0"):
        load(3).wait()
        make_q(0)
        ask(0)

    with jax.named_scope("kv1"):
        make_v(1, tp)
        forward(send_v, 1, tp)
        make_k(1, 1 - tp)
        forward(send_k, 1, 1 - tp)
        make_v(1, 1 - tp)
        forward(send_v, 1, 1 - tp)

    with jax.named_scope("q1"):
        make_q(1)

    with jax.named_scope("bias"):
        jk = iota((T, T), 0)
        jq = iota((T, T), 1)
        same = ((jq - jk) & (FAR_DILATION // MIDDLE_DILATION - 1)) == 0
        far = jnp.where(same, 0.0, NEG)
        bias2[...] = far
        bias3[0] = jnp.where(same & (jk >= jq), 0.0, NEG) + jnp.where(before[1], 0.0, NEG)
        bias3[1] = far

        @pl.loop(0, 2 * G)
        def _(b):
            which = lax.shift_right_logical(b, 2)
            gk = b & (G - 1)

            @pl.loop(0, G)
            def _(gq):
                k_pos = (iota((T, T), 0) - T * (1 - which)) * G + gk
                d = iota((T, T), 1) * G + gq - k_pos
                ok = d >= 0
                near = jnp.where(ok & (d <= REACH_STEPS), 1, 0)
                mid = jnp.where(ok & (d <= REACH_STEPS * MIDDLE_DILATION) & ((d & (MIDDLE_DILATION - 1)) == 0), 1, 0)
                wide = jnp.where(ok & (d <= REACH_STEPS * FAR_DILATION) & ((d & (FAR_DILATION - 1)) == 0), 1, 0)
                times = near + mid + wide
                value = jnp.where(times == 3, math.log2(3.0), jnp.where(times == 2, 1.0, jnp.where(times == 1, 0.0, NEG)))
                value = value + jnp.where((which == 1) | before[1], 0.0, NEG)
                bias[gq, which, pl.ds(pl.multiple_of(gk * T, T), T), :] = value

    def pass_on(i):
        @pl.when(before[1] & after[1])
        def _():
            send_q1(i).wait_recv()

            @pl.when(before[2])
            def _():
                send_q3(i).start()

    with jax.named_scope("fwdq"):
        @pl.loop(0, half)
        def _(i):
            pass_on(i)

        ask(1)

        @pl.loop(0, G)
        def _(g):
            t = g * T + iota((T, ROWS), 0)
            s = iota((T, ROWS), 1)
            perm_out[pl.ds(pl.multiple_of(g * T, T), T), :] = jnp.where(
                s == (t & (G - 1)) * T + lax.shift_right_logical(t, 2), 1.0, 0.0).astype(BF16)

        for h in range(heads):
            v0t[h] = v0[h].reshape(ROWS, HEAD).T

    def softmax_of(scores):
        top = functools.reduce(jnp.maximum, [jnp.max(s, axis=0, keepdims=True) for s in scores])
        ps = [jnp.exp2(s - top) for s in scores]
        total = functools.reduce(jnp.add, [jnp.sum(p, axis=0, keepdims=True) for p in ps])
        return top, total, [p.astype(BF16) for p in ps]

    def scores_of(keys, queries, b):
        return lax.dot_general(keys, queries, NT, preferred_element_type=F32) * SCALE + b

    def tile(g):
        return pl.ds(pl.multiple_of(g * T, T), T)

    def rows_of(ref, *where):
        return ref[where].reshape(-1, HEAD)

    def context(h):
        @pl.when(before[1])
        def _():
            for u in range(2):
                send_k(h, u).wait_recv()
                send_v(h, u).wait_recv()

        v1t[h] = rows_of(v1, h).T

    def widest(i):
        h = lax.div(i, 2)

        @pl.when(after[3])
        def _():
            send_q3(i).wait_recv()
            for s in range(2):
                t = 2 * i + s
                g = t - h * G
                q = rows_of(q3, t)
                top, total, (p4, p3) = softmax_of([
                    scores_of(rows_of(k1, h, g), q, bias3[0]),
                    scores_of(rows_of(k0, h, g), q, bias3[1])])
                o = (jnp.dot(v1t[h, :, tile(g)], p4, preferred_element_type=F32)
                     + jnp.dot(v0t[h, :, tile(g)], p3, preferred_element_type=F32))
                o3[t] = (o * (1.0 / total)).astype(BF16)
                l3[t] = top + jnp.log2(total)
            for copy in send_o3(i):
                copy.start()

    def local(h):
        @pl.loop(0, G)
        def _(g):
            q = rows_of(q0, h * G + g)
            top, total, (p_prev, p_own) = softmax_of([
                scores_of(rows_of(k1, h), q, bias[g, 0]), scores_of(rows_of(k0, h), q, bias[g, 1])])
            o = (jnp.dot(v1t[h], p_prev, preferred_element_type=F32)
                 + jnp.dot(v0t[h], p_own, preferred_element_type=F32))
            loc_o[h * G + g] = o
            loc_m[h * G + g] = top
            loc_l[h * G + g] = total

    def answer(i):
        @pl.when(before[1] & after[1])
        def _():
            @pl.when(before[2])
            def _():
                for copy in send_o3(i):
                    copy.wait_recv()

            h = lax.div(i, 2)
            for s in range(2):
                t = 2 * i + s
                g = t - h * G
                top, total, (p2,) = softmax_of([scores_of(rows_of(k1, h, g), rows_of(q1, t), bias2[...])])
                o = jnp.dot(v1t[h, :, tile(g)], p2, preferred_element_type=F32)
                lse = l3_in[t]
                peak = jnp.maximum(top, lse)
                here = jnp.exp2(top - peak)
                there = jnp.exp2(lse - peak)
                whole = total * here + there
                o1[t] = (o * (here / whole) + o3_in[t].astype(F32) * (there / whole)).astype(BF16)
                l1[t] = peak + jnp.log2(whole)
            for copy in send_o1(i):
                copy.start()

    with jax.named_scope("ctx01_o3"):
        @pl.loop(0, heads // 2)
        def _(h):
            context(h)
            for s in range(2):
                widest(2 * h + s)

    with jax.named_scope("local01_fwd"):
        @pl.loop(0, heads // 2)
        def _(h):
            local(h)
            for s in range(2):
                pass_on(half + 2 * h + s)

    with jax.named_scope("ctx23_local"):
        @pl.loop(heads // 2, heads)
        def _(h):
            context(h)
            local(h)

    with jax.named_scope("o1_o3"):
        @pl.loop(0, half)
        def _(i):
            answer(i)
            widest(half + i)

    def row_block(b):
        return slice(b * T, (b + 1) * T)

    def term(u, h, b):
        start = pl.multiple_of(u * width + h * HEAD, HEAD)
        return jnp.dot(mixed[u, h, row_block(b), :], wo_v[pl.ds(start, HEAD), :], preferred_element_type=F32)

    def finish(h):
        with jax.named_scope(f"head{h}"):
            @pl.when(before[2])
            def _():
                for i in (2 * h, 2 * h + 1):
                    for copy in send_o1(i):
                        copy.wait_recv()

            for g in range(G):
                t = h * G + g
                top, lse = loc_m[t], l1_in[t]
                peak = jnp.maximum(top, lse)
                here = jnp.exp2(top - peak)
                there = jnp.exp2(lse - peak)
                whole = loc_l[t] * here + there
                o = loc_o[t] * (here / whole) + o1_in[t].astype(F32) * (there / whole)
                mix_t[h, :, g * T:(g + 1) * T] = o.astype(BF16)
            mixed[tp, h] = lax.dot_general(perm_out[...], mix_t[h], NT, preferred_element_type=F32).astype(BF16)
            send_mixed(h).start()
        with jax.named_scope(f"acc{h}"):
            for b in range(G):
                y = term(tp, h, b)
                acc[row_block(b)] = y if h == 0 else acc[row_block(b)] + y
            if h > 0:
                send_mixed(h - 1).wait_recv()
                for b in range(G):
                    acc[row_block(b)] += term(1 - tp, h - 1, b)

    load(4).wait()
    with jax.named_scope("final"):
        finish(0)
    with jax.named_scope("o1b"):
        for i in (half, half + 1):
            answer(jnp.int32(i))
    with jax.named_scope("finalb"):
        finish(1)
    with jax.named_scope("o1c"):
        for i in range(half + 2, chunks):
            answer(jnp.int32(i))
    with jax.named_scope("finalc"):
        for h in range(2, heads):
            finish(h)

    with jax.named_scope("out"):
        send_mixed(heads - 1).wait_recv()
        for b in range(G):
            out_v[row_block(b)] = (acc[row_block(b)] + term(1 - tp, heads - 1, b)).astype(BF16)
            send_out(b).start()

    with jax.named_scope("drain"):
        send_tokens().wait_send()

        @pl.when(after[1])
        def _():
            for h in range(heads):
                for u in range(2):
                    send_k(h, u).wait_send()
                    send_v(h, u).wait_send()

        @pl.loop(0, chunks)
        def _(i):
            @pl.when(before[2])
            def _():
                send_q1(i).wait_send()

            @pl.when(before[2] & after[1])
            def _():
                send_q3(i).wait_send()

            @pl.when(after[3])
            def _():
                for copy in send_o3(i):
                    copy.wait_send()

            @pl.when(before[1] & after[1])
            def _():
                for copy in send_o1(i):
                    copy.wait_send()

        for h in range(heads):
            send_mixed(h).wait_send()
        for b in range(G):
            send_out(b).wait()


def body(tokens, query_weight, key_weight, value_weight, output_weight):
    n = lax.axis_size("sp")
    half_rows, depth = tokens.shape
    width = query_weight.shape[1]
    heads = width // HEAD
    tiles, chunks = heads * G, 2 * heads
    features = output_weight.shape[1]
    assert 2 * half_rows == ROWS and FAR_DILATION == MIDDLE_DILATION**2 and heads % 2 == 0
    assert output_weight.shape[0] == 2 * width
    vmem = pltpu.VMEM
    dma = pltpu.SemaphoreType.DMA
    split = (tiles, 2, T // 2, HEAD)
    by_head = (heads, G, 2, T // 2, HEAD)
    turned = (heads, HEAD, ROWS)
    square = (tiles, T, HEAD)
    stat = (tiles, 1, T)
    scratch = [
        vmem((2, half_rows, depth), BF16), vmem((2, half_rows, depth), BF16),
        vmem((depth, width), BF16), vmem((depth, width), BF16), vmem((depth, width), BF16),
        vmem((2 * width, features), BF16), vmem((ROWS, features), BF16), vmem((ROWS, features), F32),
        vmem((2, half_rows, HEAD), F32), vmem((2, half_rows, HEAD), F32),
        vmem((G, 2, ROWS, T), F32), vmem((T, T), F32), vmem((2, T, T), F32),
        vmem((half_rows, half_rows), BF16), vmem((ROWS, ROWS), BF16),
        vmem(split, BF16),
        vmem(by_head, BF16), vmem(by_head, BF16), vmem(by_head, BF16), vmem(by_head, BF16),
        vmem(turned, BF16), vmem(turned, BF16),
        vmem(split, BF16), vmem(split, BF16),
        vmem(square, BF16), vmem(stat, F32), vmem(square, BF16), vmem(stat, F32),
        vmem(square, BF16), vmem(stat, F32), vmem(square, BF16), vmem(stat, F32),
        vmem(square, F32), vmem(stat, F32), vmem(stat, F32),
        vmem(turned, BF16), vmem((2, heads, ROWS, HEAD), BF16),
        dma((5,)), dma((2, 1)), dma((2, chunks)), dma((2, chunks)), dma((2, chunks)), dma((2, chunks)),
        dma((2, chunks)), dma((2, chunks)), dma((2, chunks)), dma((2, chunks)), dma((2, heads)), dma((G,)),
    ]
    hbm = pl.BlockSpec(memory_space=pltpu.HBM)
    return pl.pallas_call(
        functools.partial(kernel, n),
        out_shape=jax.ShapeDtypeStruct((ROWS, features), BF16),
        in_specs=[hbm] * 5,
        out_specs=pl.BlockSpec(memory_space=pl.ANY),
        scratch_shapes=scratch,
        compiler_params=pltpu.CompilerParams(
            collective_id=0, has_side_effects=True, vmem_limit_bytes=VMEM_LIMIT),
        name="attention",
    )(tokens, query_weight, key_weight, value_weight, output_weight)


def solution(mesh):
    in_specs = (
        P(("grp", "sp", "tp"), None),
        P(None, "tp"),
        P(None, "tp"),
        P(None, "tp"),
        P(None, "tp"),
    )
    out_specs = P(("grp", "sp"), "tp")
    return jax.shard_map(body, mesh=mesh, in_specs=in_specs, out_specs=out_specs, check_vma=False)
```

```python
import functools
import math

import jax
import jax.numpy as jnp
from jax import lax
from jax.experimental import pallas as pl
from jax.experimental.pallas import tpu as pltpu
from jax.sharding import PartitionSpec as P

HEAD = 128
REACH_STEPS = 128
MIDDLE_DILATION = 4
FAR_DILATION = 16
THETA_BASE = 500000.0

MESH = pl.DeviceIdType.MESH
F32 = jnp.float32
BF16 = jnp.bfloat16
G = MIDDLE_DILATION
T = REACH_STEPS
ROWS = G * T
NEG = -1e30
VMEM_LIMIT = 55_000_000
SCALE = HEAD**-0.5 * math.log2(math.e)
NT = (((1,), (1,)), ((), ()))


def iota(shape, dim):
    return lax.broadcasted_iota(jnp.int32, shape, dim)


def sin_cos(x):
    n = jnp.floor(x * (2.0 / math.pi) + 0.5)
    r = ((x - n * 1.5703125) - n * 4.837512969970703125e-4) - n * 7.549789954891882e-8
    z = r * r
    s = r + r * z * ((-1.9515295891e-4 * z + 8.3321608736e-3) * z - 1.6666654611e-1)
    c = 1.0 - 0.5 * z + z * z * ((2.443315711809948e-5 * z - 1.388731625493765e-3) * z + 4.166664568298827e-2)
    k = n.astype(jnp.int32) & 3
    odd = (k & 1) == 1
    sine = jnp.where(odd, c, s)
    cosine = jnp.where(odd, s, c)
    sine = jnp.where((k & 2) == 2, -sine, sine)
    cosine = jnp.where(((k + 1) & 2) == 2, -cosine, cosine)
    return sine, cosine


def kernel(n, tokens, wq, wk, wv, wo, out,
           x_nat, x, wq_v, wk_v, wv_v, wo_v, out_v, acc,
           rope_c, rope_s, bias, bias2, bias3, perm_in, perm_out,
           q0, k0, v0, k1, v1, v0t, v1t, q1, q3, qx, ox, lx,
           o3, l3, o3_in, l3_in, o1, l1, o1_in, l1_in,
           loc_o, loc_m, loc_l, mix_t, mixed,
           load_sem, tok_sem, k_sem, v_sem, q1_sem, q3_sem,
           o3_sem, l3_sem, o1_sem, l1_sem, qx_sem, ox_sem, mix_sem, out_sem):
    c = lax.axis_index("sp")
    tp = lax.axis_index("tp")
    heads = k0.shape[0]
    width = heads * HEAD
    chunks = 2 * heads
    pairs = heads // 2
    half_rows = ROWS // 2
    piece = T // 2
    partner = {"tp": 1 - tp}

    before = [None, c >= 1, c >= 2, c >= 3]
    after = [None, c + 1 < n, c + 2 < n, c + 3 < n]

    def at(distance):
        return {"sp": jnp.clip(c + distance, 0, n - 1)}

    def load(i):
        src, dst = ((tokens, x_nat.at[tp]), (wk, wk_v), (wv, wv_v), (wq, wq_v), (wo, wo_v))[i]
        return pltpu.make_async_copy(src, dst, load_sem.at[i])

    for i in range(5):
        load(i).start()

    barrier = pltpu.get_barrier_semaphore()

    def greet(device):
        pl.semaphore_signal(barrier, inc=1, device_id=device, device_id_type=MESH)

    greet(partner)
    pl.when(before[1])(functools.partial(greet, at(-1)))
    pl.when(before[3])(functools.partial(greet, at(-2)))
    pl.when(before[1] & after[1])(functools.partial(greet, at(1)))
    pl.when(before[1] & after[2])(functools.partial(greet, at(2)))

    def remote(src, dst, sems, i, device):
        return pltpu.make_async_remote_copy(
            src_ref=src, dst_ref=dst, send_sem=sems.at[0, i], recv_sem=sems.at[1, i],
            device_id=device, device_id_type=MESH)

    def send_tokens():
        return remote(tokens, x_nat.at[tp], tok_sem, 0, partner)

    def send_k(h, u):
        return remote(k0.at[h, :, u], k1.at[h, :, u], k_sem, 2 * h + u, at(1))

    def send_v(h, u):
        return remote(v0.at[h, :, u], v1.at[h, :, u], v_sem, 2 * h + u, at(1))

    def chunk(ref, i):
        return ref.at[pl.ds(2 * i, 2)]

    def send_q1(i):
        return remote(chunk(q0, i), chunk(q1, i), q1_sem, i, at(-1))

    def send_q3(i):
        return remote(chunk(q1, i), chunk(q3, i), q3_sem, i, at(-2))

    def send_qx(i):
        return remote(chunk(q1, i), chunk(qx, i), qx_sem, i, at(-1))

    def send_ox(i):
        return tuple(
            pltpu.make_async_remote_copy(
                src_ref=chunk(src, i), dst_ref=chunk(dst, i), send_sem=ox_sem.at[k, i], recv_sem=sems.at[1, i],
                device_id=at(1), device_id_type=MESH)
            for k, (src, dst, sems) in enumerate(((ox, o3_in, o3_sem), (lx, l3_in, l3_sem))))

    def send_o3(i):
        return (remote(chunk(o3, i), chunk(o3_in, i), o3_sem, i, at(2)),
                remote(chunk(l3, i), chunk(l3_in, i), l3_sem, i, at(2)))

    def send_o1(i):
        return (remote(chunk(o1, i), chunk(o1_in, i), o1_sem, i, at(1)),
                remote(chunk(l1, i), chunk(l1_in, i), l1_sem, i, at(1)))

    def send_mixed(h):
        return remote(mixed.at[tp, h], mixed.at[tp, h], mix_sem, h, partner)

    def send_out(b):
        rows = pl.ds(b * T, T)
        return pltpu.make_async_copy(out_v.at[rows], out.at[rows], out_sem.at[b])

    with jax.named_scope("tables"):
        row = iota((half_rows, half_rows), 0)
        col = iota((half_rows, half_rows), 1)
        perm_in[...] = jnp.where(row == (col & (G - 1)) * piece + lax.shift_right_logical(col, 2), 1.0, 0.0).astype(BF16)

        lane = iota((T, HEAD), 1)
        index = lane & (HEAD // 2 - 1)
        inverse = jnp.ones((T, HEAD), F32)
        for bit in range(6):
            factor = THETA_BASE ** (-(2.0**bit) / (HEAD // 2))
            inverse = jnp.where((lax.shift_right_logical(index, bit) & 1) == 1, inverse * factor, inverse)

        @pl.loop(0, 4)
        def _(i):
            u = lax.shift_right_logical(i, 1)
            r = iota((T, HEAD), 0) + (i & 1) * T
            local = (r & (piece - 1)) * G + lax.shift_right_logical(r, 6)
            position = c * ROWS + u * half_rows + local
            sine, cosine = sin_cos(position.astype(F32) * inverse)
            rows = pl.ds(pl.multiple_of((i & 1) * T, T), T)
            rope_c[u, rows, :] = cosine
            rope_s[u, rows, :] = jnp.where(lane < HEAD // 2, -sine, sine)

    def permuted(u):
        x[u] = jnp.dot(perm_in[...], x_nat[u], preferred_element_type=F32).astype(BF16)

    def columns(p):
        return slice(2 * p * HEAD, (2 * p + 2) * HEAD)

    def rotated(y, u):
        return (y * rope_c[u] + pltpu.roll(y, HEAD // 2, 1) * rope_s[u]).astype(BF16)

    def project(w, p, u):
        return jnp.dot(x[u], w[:, columns(p)], preferred_element_type=F32)

    def make_k(p, u):
        y = project(wk_v, p, u)
        for s in range(2):
            z = rotated(y[:, s * HEAD:(s + 1) * HEAD], u)
            for g in range(G):
                k0[2 * p + s, g, u] = z[g * piece:(g + 1) * piece]

    def make_v(p, u):
        y = project(wv_v, p, u).astype(BF16)
        for s in range(2):
            for g in range(G):
                v0[2 * p + s, g, u] = y[g * piece:(g + 1) * piece, s * HEAD:(s + 1) * HEAD]

    def forward(send, p, u):
        @pl.when(after[1])
        def _():
            for s in range(2):
                send(2 * p + s, u).start()

    with jax.named_scope("own_k"):
        load(0).wait()
        permuted(tp)
        load(1).wait()
        make_k(0, tp)

    with jax.named_scope("barrier"):
        count = 1
        for exists in (after[1], before[2], before[1] & after[2], before[3]):
            count = count + exists.astype(jnp.int32)
        pl.semaphore_wait(barrier, count)
        send_tokens().start()

    with jax.named_scope("own_kv"):
        forward(send_k, 0, tp)
        load(2).wait()
        make_v(0, tp)
        forward(send_v, 0, tp)

    @pl.when(c < 1)
    def _():
        k1[...] = jnp.zeros_like(k1)
        v1[...] = jnp.zeros_like(v1)

    @pl.when(c < 2)
    def _():
        o3_in[...] = jnp.zeros_like(o3_in)
        l3_in[...] = jnp.full_like(l3_in, NEG)
        o1_in[...] = jnp.zeros_like(o1_in)
        l1_in[...] = jnp.full_like(l1_in, NEG)

    def make_q(p):
        y = jnp.dot(x[...].reshape(ROWS, x.shape[2]), wq_v[:, columns(p)], preferred_element_type=F32)
        for s in range(2):
            for u in range(2):
                z = rotated(y[u * half_rows:(u + 1) * half_rows, s * HEAD:(s + 1) * HEAD], u)
                for g in range(G):
                    q0[(2 * p + s) * G + g, u] = z[g * piece:(g + 1) * piece]

    half = chunks // 2

    def ask(p):
        @pl.when(before[2])
        def _():
            for i in range(p * half, (p + 1) * half):
                send_q1(i).start()

    with jax.named_scope("own_kv1"):
        make_k(1, tp)

    with jax.named_scope("tokwait"):
        send_tokens().wait_recv()

    with jax.named_scope("other_kv0"):
        permuted(1 - tp)
        make_k(0, 1 - tp)
        forward(send_k, 0, 1 - tp)
        make_v(0, 1 - tp)
        forward(send_v, 0, 1 - tp)
        forward(send_k, 1, tp)

    with jax.named_scope("q0"):
        load(3).wait()
        make_q(0)
        ask(0)

    with jax.named_scope("kv1"):
        make_v(1, tp)
        forward(send_v, 1, tp)
        make_k(1, 1 - tp)
        forward(send_k, 1, 1 - tp)
        make_v(1, 1 - tp)
        forward(send_v, 1, 1 - tp)

    with jax.named_scope("q1"):
        make_q(1)

    with jax.named_scope("bias"):
        jk = iota((T, T), 0)
        jq = iota((T, T), 1)
        same = ((jq - jk) & (FAR_DILATION // MIDDLE_DILATION - 1)) == 0
        far = jnp.where(same, 0.0, NEG)
        bias2[...] = far
        bias3[0] = jnp.where(same & (jk >= jq), 0.0, NEG) + jnp.where(before[1], 0.0, NEG)
        bias3[1] = far

        @pl.loop(0, 2 * G)
        def _(b):
            which = lax.shift_right_logical(b, 2)
            gk = b & (G - 1)

            @pl.loop(0, G)
            def _(gq):
                k_pos = (iota((T, T), 0) - T * (1 - which)) * G + gk
                d = iota((T, T), 1) * G + gq - k_pos
                ok = d >= 0
                near = jnp.where(ok & (d <= REACH_STEPS), 1, 0)
                mid = jnp.where(ok & (d <= REACH_STEPS * MIDDLE_DILATION) & ((d & (MIDDLE_DILATION - 1)) == 0), 1, 0)
                wide = jnp.where(ok & (d <= REACH_STEPS * FAR_DILATION) & ((d & (FAR_DILATION - 1)) == 0), 1, 0)
                times = near + mid + wide
                value = jnp.where(times == 3, math.log2(3.0), jnp.where(times == 2, 1.0, jnp.where(times == 1, 0.0, NEG)))
                value = value + jnp.where((which == 1) | before[1], 0.0, NEG)
                bias[gq, which, pl.ds(pl.multiple_of(gk * T, T), T), :] = value

    def pass_on(i):
        @pl.when(before[1] & after[1])
        def _():
            send_q1(i).wait_recv()

            @pl.when(before[3])
            def _():
                send_q3(i).start()

            @pl.when(c == 2)
            def _():
                send_qx(i).start()

    with jax.named_scope("fwdq"):
        @pl.loop(0, half)
        def _(i):
            pass_on(i)

        ask(1)

        @pl.loop(0, G)
        def _(g):
            t = g * T + iota((T, ROWS), 0)
            s = iota((T, ROWS), 1)
            perm_out[pl.ds(pl.multiple_of(g * T, T), T), :] = jnp.where(
                s == (t & (G - 1)) * T + lax.shift_right_logical(t, 2), 1.0, 0.0).astype(BF16)

        for h in range(heads):
            v0t[h] = v0[h].reshape(ROWS, HEAD).T

    def softmax_of(scores):
        top = functools.reduce(jnp.maximum, [jnp.max(s, axis=0, keepdims=True) for s in scores])
        ps = [jnp.exp2(s - top) for s in scores]
        total = functools.reduce(jnp.add, [jnp.sum(p, axis=0, keepdims=True) for p in ps])
        return top, total, [p.astype(BF16) for p in ps]

    def scores_of(keys, queries, b):
        return lax.dot_general(keys, queries, NT, preferred_element_type=F32) * SCALE + b

    def tile(g):
        return pl.ds(pl.multiple_of(g * T, T), T)

    def rows_of(ref, *where):
        return ref[where].reshape(-1, HEAD)

    def context(h):
        @pl.when(before[1])
        def _():
            for u in range(2):
                send_k(h, u).wait_recv()
                send_v(h, u).wait_recv()

        v1t[h] = rows_of(v1, h).T

    def widest(i):
        h = lax.div(i, 2)

        @pl.when(before[1] & after[3])
        def _():
            send_q3(i).wait_recv()
            for s in range(2):
                t = 2 * i + s
                g = t - h * G
                q = rows_of(q3, t)
                top, total, (p4, p3) = softmax_of([
                    scores_of(rows_of(k1, h, g), q, bias3[0]),
                    scores_of(rows_of(k0, h, g), q, bias3[1])])
                o = (jnp.dot(v1t[h, :, tile(g)], p4, preferred_element_type=F32)
                     + jnp.dot(v0t[h, :, tile(g)], p3, preferred_element_type=F32))
                o3[t] = (o * (1.0 / total)).astype(BF16)
                l3[t] = top + jnp.log2(total)
            for copy in send_o3(i):
                copy.start()

    def extra(i):
        h = lax.div(i, 2)

        @pl.when((c == 1) & after[2])
        def _():
            send_qx(i).wait_recv()
            for s in range(2):
                t = 2 * i + s
                g = t - h * G
                top, total, (p3,) = softmax_of([scores_of(rows_of(k1, h, g), rows_of(qx, t), bias2[...])])
                o = jnp.dot(v1t[h, :, tile(g)], p3, preferred_element_type=F32)
                ox[t] = (o * (1.0 / total)).astype(BF16)
                lx[t] = top + jnp.log2(total)
            for copy in send_ox(i):
                copy.start()

    def local(h):
        @pl.loop(0, G)
        def _(g):
            q = rows_of(q0, h * G + g)
            top, total, (p_prev, p_own) = softmax_of([
                scores_of(rows_of(k1, h), q, bias[g, 0]), scores_of(rows_of(k0, h), q, bias[g, 1])])
            o = (jnp.dot(v1t[h], p_prev, preferred_element_type=F32)
                 + jnp.dot(v0t[h], p_own, preferred_element_type=F32))
            loc_o[h * G + g] = o
            loc_m[h * G + g] = top
            loc_l[h * G + g] = total

    def answer(i):
        @pl.when(before[1] & after[1])
        def _():
            @pl.when(before[2])
            def _():
                for copy in send_o3(i):
                    copy.wait_recv()

            h = lax.div(i, 2)
            for s in range(2):
                t = 2 * i + s
                g = t - h * G
                top, total, (p2,) = softmax_of([scores_of(rows_of(k1, h, g), rows_of(q1, t), bias2[...])])
                o = jnp.dot(v1t[h, :, tile(g)], p2, preferred_element_type=F32)
                lse = l3_in[t]
                peak = jnp.maximum(top, lse)
                here = jnp.exp2(top - peak)
                there = jnp.exp2(lse - peak)
                whole = total * here + there
                o1[t] = (o * (here / whole) + o3_in[t].astype(F32) * (there / whole)).astype(BF16)
                l1[t] = peak + jnp.log2(whole)
            for copy in send_o1(i):
                copy.start()

    with jax.named_scope("ctx01_o3"):
        @pl.loop(0, heads // 2)
        def _(h):
            context(h)
            for s in range(2):
                widest(2 * h + s)
                extra(2 * h + s)

    with jax.named_scope("local01_fwd"):
        @pl.loop(0, heads // 2)
        def _(h):
            local(h)
            for s in range(2):
                pass_on(half + 2 * h + s)

    with jax.named_scope("ctx23_local"):
        @pl.loop(heads // 2, heads)
        def _(h):
            context(h)
            local(h)

    with jax.named_scope("o1_o3"):
        @pl.loop(0, half)
        def _(i):
            answer(i)
            widest(half + i)
            extra(half + i)

    def row_block(b):
        return slice(b * T, (b + 1) * T)

    def term(u, h, b):
        start = pl.multiple_of(u * width + h * HEAD, HEAD)
        return jnp.dot(mixed[u, h, row_block(b), :], wo_v[pl.ds(start, HEAD), :], preferred_element_type=F32)

    def finish(h):
        with jax.named_scope(f"head{h}"):
            @pl.when(before[2])
            def _():
                for i in (2 * h, 2 * h + 1):
                    for copy in send_o1(i):
                        copy.wait_recv()

            for g in range(G):
                t = h * G + g
                top, lse = loc_m[t], l1_in[t]
                peak = jnp.maximum(top, lse)
                here = jnp.exp2(top - peak)
                there = jnp.exp2(lse - peak)
                whole = loc_l[t] * here + there
                o = loc_o[t] * (here / whole) + o1_in[t].astype(F32) * (there / whole)
                mix_t[h, :, g * T:(g + 1) * T] = o.astype(BF16)
            mixed[tp, h] = lax.dot_general(perm_out[...], mix_t[h], NT, preferred_element_type=F32).astype(BF16)
            send_mixed(h).start()
        with jax.named_scope(f"acc{h}"):
            for b in range(G):
                y = term(tp, h, b)
                acc[row_block(b)] = y if h == 0 else acc[row_block(b)] + y
            if h < heads - 1:
                send_mixed(h).wait_recv()
                for b in range(G):
                    acc[row_block(b)] += term(1 - tp, h, b)

    load(4).wait()
    with jax.named_scope("final"):
        finish(0)
    with jax.named_scope("o1b"):
        for i in (half, half + 1):
            answer(jnp.int32(i))
    with jax.named_scope("finalb"):
        finish(1)
    with jax.named_scope("o1c"):
        for i in range(half + 2, chunks):
            answer(jnp.int32(i))
    with jax.named_scope("finalc"):
        for h in range(2, heads):
            finish(h)

    with jax.named_scope("out"):
        send_mixed(heads - 1).wait_recv()
        for b in range(G):
            out_v[row_block(b)] = (acc[row_block(b)] + term(1 - tp, heads - 1, b)).astype(BF16)
            send_out(b).start()

    with jax.named_scope("drain"):
        send_tokens().wait_send()

        @pl.when(after[1])
        def _():
            for h in range(heads):
                for u in range(2):
                    send_k(h, u).wait_send()
                    send_v(h, u).wait_send()

        @pl.loop(0, chunks)
        def _(i):
            @pl.when(before[2])
            def _():
                send_q1(i).wait_send()

            @pl.when(before[3] & after[1])
            def _():
                send_q3(i).wait_send()

            @pl.when((c == 2) & after[1])
            def _():
                send_qx(i).wait_send()

            @pl.when((c == 1) & after[2])
            def _():
                for copy in send_ox(i):
                    copy.wait_send()

            @pl.when(before[1] & after[3])
            def _():
                for copy in send_o3(i):
                    copy.wait_send()

            @pl.when(before[1] & after[1])
            def _():
                for copy in send_o1(i):
                    copy.wait_send()

        for h in range(heads):
            send_mixed(h).wait_send()
        for b in range(G):
            send_out(b).wait()


def body(tokens, query_weight, key_weight, value_weight, output_weight):
    n = lax.axis_size("sp")
    half_rows, depth = tokens.shape
    width = query_weight.shape[1]
    heads = width // HEAD
    tiles, chunks = heads * G, 2 * heads
    features = output_weight.shape[1]
    assert 2 * half_rows == ROWS and FAR_DILATION == MIDDLE_DILATION**2 and heads % 2 == 0
    assert output_weight.shape[0] == 2 * width
    vmem = pltpu.VMEM
    dma = pltpu.SemaphoreType.DMA
    split = (tiles, 2, T // 2, HEAD)
    by_head = (heads, G, 2, T // 2, HEAD)
    turned = (heads, HEAD, ROWS)
    square = (tiles, T, HEAD)
    stat = (tiles, 1, T)
    scratch = [
        vmem((2, half_rows, depth), BF16), vmem((2, half_rows, depth), BF16),
        vmem((depth, width), BF16), vmem((depth, width), BF16), vmem((depth, width), BF16),
        vmem((2 * width, features), BF16), vmem((ROWS, features), BF16), vmem((ROWS, features), F32),
        vmem((2, half_rows, HEAD), F32), vmem((2, half_rows, HEAD), F32),
        vmem((G, 2, ROWS, T), F32), vmem((T, T), F32), vmem((2, T, T), F32),
        vmem((half_rows, half_rows), BF16), vmem((ROWS, ROWS), BF16),
        vmem(split, BF16),
        vmem(by_head, BF16), vmem(by_head, BF16), vmem(by_head, BF16), vmem(by_head, BF16),
        vmem(turned, BF16), vmem(turned, BF16),
        vmem(split, BF16), vmem(split, BF16), vmem(split, BF16), vmem(square, BF16), vmem(stat, F32),
        vmem(square, BF16), vmem(stat, F32), vmem(square, BF16), vmem(stat, F32),
        vmem(square, BF16), vmem(stat, F32), vmem(square, BF16), vmem(stat, F32),
        vmem(square, F32), vmem(stat, F32), vmem(stat, F32),
        vmem(turned, BF16), vmem((2, heads, ROWS, HEAD), BF16),
        dma((5,)), dma((2, 1)), dma((2, chunks)), dma((2, chunks)), dma((2, chunks)), dma((2, chunks)),
        dma((2, chunks)), dma((2, chunks)), dma((2, chunks)), dma((2, chunks)), dma((2, chunks)), dma((2, chunks)), dma((2, heads)), dma((G,)),
    ]
    hbm = pl.BlockSpec(memory_space=pltpu.HBM)
    return pl.pallas_call(
        functools.partial(kernel, n),
        out_shape=jax.ShapeDtypeStruct((ROWS, features), BF16),
        in_specs=[hbm] * 5,
        out_specs=pl.BlockSpec(memory_space=pl.ANY),
        scratch_shapes=scratch,
        compiler_params=pltpu.CompilerParams(
            collective_id=0, has_side_effects=True, vmem_limit_bytes=VMEM_LIMIT),
        name="attention",
    )(tokens, query_weight, key_weight, value_weight, output_weight)


def solution(mesh):
    in_specs = (
        P(("grp", "sp", "tp"), None),
        P(None, "tp"),
        P(None, "tp"),
        P(None, "tp"),
        P(None, "tp"),
    )
    out_specs = P(("grp", "sp"), "tp")
    return jax.shard_map(body, mesh=mesh, in_specs=in_specs, out_specs=out_specs, check_vma=False)
```

```python
import functools
import math

import jax
import jax.numpy as jnp
from jax import lax
from jax.experimental import pallas as pl
from jax.experimental.pallas import tpu as pltpu
from jax.sharding import PartitionSpec as P

HEAD = 128
REACH_STEPS = 128
MIDDLE_DILATION = 4
FAR_DILATION = 16
THETA_BASE = 500000.0

MESH = pl.DeviceIdType.MESH
F32 = jnp.float32
BF16 = jnp.bfloat16
G = MIDDLE_DILATION
T = REACH_STEPS
ROWS = G * T
NEG = -1e30
VMEM_LIMIT = 55_000_000
SCALE = HEAD**-0.5 * math.log2(math.e)
NT = (((1,), (1,)), ((), ()))


def iota(shape, dim):
    return lax.broadcasted_iota(jnp.int32, shape, dim)


def sin_cos(x):
    n = jnp.floor(x * (2.0 / math.pi) + 0.5)
    r = ((x - n * 1.5703125) - n * 4.837512969970703125e-4) - n * 7.549789954891882e-8
    z = r * r
    s = r + r * z * ((-1.9515295891e-4 * z + 8.3321608736e-3) * z - 1.6666654611e-1)
    c = 1.0 - 0.5 * z + z * z * ((2.443315711809948e-5 * z - 1.388731625493765e-3) * z + 4.166664568298827e-2)
    k = n.astype(jnp.int32) & 3
    odd = (k & 1) == 1
    sine = jnp.where(odd, c, s)
    cosine = jnp.where(odd, s, c)
    sine = jnp.where((k & 2) == 2, -sine, sine)
    cosine = jnp.where(((k + 1) & 2) == 2, -cosine, cosine)
    return sine, cosine


def kernel(n, tokens, wq, wk, wv, wo, out,
           x_nat, x, wq_v, wk_v, wv_v, wo_v, out_v, acc,
           rope_c, rope_s, bias, bias2, bias3, perm_in, perm_out,
           q0, k0, v0, k1, v1, v0t, v1t, q1, q3, qx, ox, lx,
           o3, l3, o3_in, l3_in, o1, l1, o1_in, l1_in,
           loc_o, loc_m, loc_l, mix_t, mixed,
           load_sem, tok_sem, k_sem, v_sem, q1_sem, q3_sem,
           o3_sem, l3_sem, o1_sem, l1_sem, qx_sem, ox_sem, mix_sem, out_sem):
    c = lax.axis_index("sp")
    tp = lax.axis_index("tp")
    heads = k0.shape[0]
    width = heads * HEAD
    chunks = 2 * heads
    pairs = heads // 2
    half_rows = ROWS // 2
    piece = T // 2
    partner = {"tp": 1 - tp}

    before = [None, c >= 1, c >= 2, c >= 3]
    after = [None, c + 1 < n, c + 2 < n, c + 3 < n]

    def at(distance):
        return {"sp": jnp.clip(c + distance, 0, n - 1)}

    def load(i):
        src, dst = ((tokens, x_nat.at[tp]), (wk, wk_v), (wv, wv_v), (wq, wq_v), (wo, wo_v))[i]
        return pltpu.make_async_copy(src, dst, load_sem.at[i])

    for i in range(5):
        load(i).start()

    barrier = pltpu.get_barrier_semaphore()

    def greet(device):
        pl.semaphore_signal(barrier, inc=1, device_id=device, device_id_type=MESH)

    greet(partner)
    pl.when(before[1])(functools.partial(greet, at(-1)))
    pl.when(before[3])(functools.partial(greet, at(-2)))
    pl.when(before[1] & after[1])(functools.partial(greet, at(1)))
    pl.when(before[1] & after[2])(functools.partial(greet, at(2)))

    def remote(src, dst, sems, i, device):
        return pltpu.make_async_remote_copy(
            src_ref=src, dst_ref=dst, send_sem=sems.at[0, i], recv_sem=sems.at[1, i],
            device_id=device, device_id_type=MESH)

    def send_tokens():
        return remote(tokens, x_nat.at[tp], tok_sem, 0, partner)

    def send_k(h, u):
        return remote(k0.at[h, :, u], k1.at[h, :, u], k_sem, 2 * h + u, at(1))

    def send_v(h, u):
        return remote(v0.at[h, :, u], v1.at[h, :, u], v_sem, 2 * h + u, at(1))

    def chunk(ref, i):
        return ref.at[pl.ds(2 * i, 2)]

    def send_q1(i):
        return remote(chunk(q0, i), chunk(q1, i), q1_sem, i, at(-1))

    def send_q3(i):
        return remote(chunk(q1, i), chunk(q3, i), q3_sem, i, at(-2))

    def send_qx(i):
        return remote(chunk(q1, i), chunk(qx, i), qx_sem, i, at(-1))

    def send_ox(i):
        return tuple(
            pltpu.make_async_remote_copy(
                src_ref=chunk(src, i), dst_ref=chunk(dst, i), send_sem=ox_sem.at[k, i], recv_sem=sems.at[1, i],
                device_id=at(1), device_id_type=MESH)
            for k, (src, dst, sems) in enumerate(((ox, o3_in, o3_sem), (lx, l3_in, l3_sem))))

    def send_o3(i):
        return (remote(chunk(o3, i), chunk(o3_in, i), o3_sem, i, at(2)),
                remote(chunk(l3, i), chunk(l3_in, i), l3_sem, i, at(2)))

    def send_o1(i):
        return (remote(chunk(o1, i), chunk(o1_in, i), o1_sem, i, at(1)),
                remote(chunk(l1, i), chunk(l1_in, i), l1_sem, i, at(1)))

    def send_mixed(h):
        return remote(mixed.at[tp, h], mixed.at[tp, h], mix_sem, h, partner)

    def send_out(b):
        rows = pl.ds(b * T, T)
        return pltpu.make_async_copy(out_v.at[rows], out.at[rows], out_sem.at[b])

    with jax.named_scope("tables"):
        row = iota((half_rows, half_rows), 0)
        col = iota((half_rows, half_rows), 1)
        perm_in[...] = jnp.where(row == (col & (G - 1)) * piece + lax.shift_right_logical(col, 2), 1.0, 0.0).astype(BF16)

        lane = iota((T, HEAD), 1)
        index = lane & (HEAD // 2 - 1)
        inverse = jnp.ones((T, HEAD), F32)
        for bit in range(6):
            factor = THETA_BASE ** (-(2.0**bit) / (HEAD // 2))
            inverse = jnp.where((lax.shift_right_logical(index, bit) & 1) == 1, inverse * factor, inverse)

        @pl.loop(0, 4)
        def _(i):
            u = lax.shift_right_logical(i, 1)
            r = iota((T, HEAD), 0) + (i & 1) * T
            local = (r & (piece - 1)) * G + lax.shift_right_logical(r, 6)
            position = c * ROWS + u * half_rows + local
            sine, cosine = sin_cos(position.astype(F32) * inverse)
            rows = pl.ds(pl.multiple_of((i & 1) * T, T), T)
            rope_c[u, rows, :] = cosine
            rope_s[u, rows, :] = jnp.where(lane < HEAD // 2, -sine, sine)

    def permuted(u):
        x[u] = jnp.dot(perm_in[...], x_nat[u], preferred_element_type=F32).astype(BF16)

    def columns(p):
        return slice(2 * p * HEAD, (2 * p + 2) * HEAD)

    def rotated(y, u):
        return (y * rope_c[u] + pltpu.roll(y, HEAD // 2, 1) * rope_s[u]).astype(BF16)

    def project(w, p, u):
        return jnp.dot(x[u], w[:, columns(p)], preferred_element_type=F32)

    def make_k(p, u):
        y = project(wk_v, p, u)
        for s in range(2):
            z = rotated(y[:, s * HEAD:(s + 1) * HEAD], u)
            for g in range(G):
                k0[2 * p + s, g, u] = z[g * piece:(g + 1) * piece]

    def make_v(p, u):
        y = project(wv_v, p, u).astype(BF16)
        for s in range(2):
            for g in range(G):
                v0[2 * p + s, g, u] = y[g * piece:(g + 1) * piece, s * HEAD:(s + 1) * HEAD]

    def forward(send, p, u):
        @pl.when(after[1])
        def _():
            for s in range(2):
                send(2 * p + s, u).start()

    with jax.named_scope("own_k"):
        load(0).wait()
        permuted(tp)
        load(1).wait()
        make_k(0, tp)

    with jax.named_scope("barrier"):
        count = 1
        for exists in (after[1], before[2], before[1] & after[2], before[3]):
            count = count + exists.astype(jnp.int32)
        pl.semaphore_wait(barrier, count)
        send_tokens().start()

    with jax.named_scope("own_kv"):
        forward(send_k, 0, tp)
        load(2).wait()
        make_v(0, tp)
        forward(send_v, 0, tp)

    @pl.when(c < 1)
    def _():
        k1[...] = jnp.zeros_like(k1)
        v1[...] = jnp.zeros_like(v1)

    @pl.when(c < 2)
    def _():
        o3_in[...] = jnp.zeros_like(o3_in)
        l3_in[...] = jnp.full_like(l3_in, NEG)
        o1_in[...] = jnp.zeros_like(o1_in)
        l1_in[...] = jnp.full_like(l1_in, NEG)

    def make_q(p):
        y = jnp.dot(x[...].reshape(ROWS, x.shape[2]), wq_v[:, columns(p)], preferred_element_type=F32)
        for s in range(2):
            for u in range(2):
                z = rotated(y[u * half_rows:(u + 1) * half_rows, s * HEAD:(s + 1) * HEAD], u)
                for g in range(G):
                    q0[(2 * p + s) * G + g, u] = z[g * piece:(g + 1) * piece]

    half = chunks // 2

    def ask(p):
        @pl.when(before[2])
        def _():
            for i in range(p * half, (p + 1) * half):
                send_q1(i).start()

    with jax.named_scope("own_kv1"):
        make_k(1, tp)

    with jax.named_scope("tokwait"):
        send_tokens().wait_recv()

    with jax.named_scope("other_kv0"):
        permuted(1 - tp)
        make_k(0, 1 - tp)
        forward(send_k, 0, 1 - tp)
        make_v(0, 1 - tp)
        forward(send_v, 0, 1 - tp)
        forward(send_k, 1, tp)

    with jax.named_scope("q0"):
        load(3).wait()
        make_q(0)
        ask(0)

    with jax.named_scope("kv1"):
        make_v(1, tp)
        forward(send_v, 1, tp)
        make_k(1, 1 - tp)
        forward(send_k, 1, 1 - tp)
        make_v(1, 1 - tp)
        forward(send_v, 1, 1 - tp)

    with jax.named_scope("q1"):
        make_q(1)

    with jax.named_scope("bias"):
        jk = iota((T, T), 0)
        jq = iota((T, T), 1)
        same = ((jq - jk) & (FAR_DILATION // MIDDLE_DILATION - 1)) == 0
        far = jnp.where(same, 0.0, NEG)
        bias2[...] = far
        bias3[0] = jnp.where(same & (jk >= jq), 0.0, NEG) + jnp.where(before[1], 0.0, NEG)
        bias3[1] = far

        @pl.loop(0, 2 * G)
        def _(b):
            which = lax.shift_right_logical(b, 2)
            gk = b & (G - 1)

            @pl.loop(0, G)
            def _(gq):
                k_pos = (iota((T, T), 0) - T * (1 - which)) * G + gk
                d = iota((T, T), 1) * G + gq - k_pos
                ok = d >= 0
                near = jnp.where(ok & (d <= REACH_STEPS), 1, 0)
                mid = jnp.where(ok & (d <= REACH_STEPS * MIDDLE_DILATION) & ((d & (MIDDLE_DILATION - 1)) == 0), 1, 0)
                wide = jnp.where(ok & (d <= REACH_STEPS * FAR_DILATION) & ((d & (FAR_DILATION - 1)) == 0), 1, 0)
                times = near + mid + wide
                value = jnp.where(times == 3, math.log2(3.0), jnp.where(times == 2, 1.0, jnp.where(times == 1, 0.0, NEG)))
                value = value + jnp.where((which == 1) | before[1], 0.0, NEG)
                bias[gq, which, pl.ds(pl.multiple_of(gk * T, T), T), :] = value

    def pass_on(i):
        @pl.when(before[1] & after[1])
        def _():
            send_q1(i).wait_recv()

            @pl.when(before[3])
            def _():
                send_q3(i).start()

            @pl.when(c == 2)
            def _():
                send_qx(i).start()

    with jax.named_scope("fwdq"):
        @pl.loop(0, half)
        def _(i):
            pass_on(i)

        ask(1)

        @pl.loop(0, G)
        def _(g):
            t = g * T + iota((T, ROWS), 0)
            s = iota((T, ROWS), 1)
            perm_out[pl.ds(pl.multiple_of(g * T, T), T), :] = jnp.where(
                s == (t & (G - 1)) * T + lax.shift_right_logical(t, 2), 1.0, 0.0).astype(BF16)

        for h in range(heads):
            v0t[h] = v0[h].reshape(ROWS, HEAD).T

    def softmax_of(scores):
        top = functools.reduce(jnp.maximum, [jnp.max(s, axis=0, keepdims=True) for s in scores])
        ps = [jnp.exp2(s - top) for s in scores]
        total = functools.reduce(jnp.add, [jnp.sum(p, axis=0, keepdims=True) for p in ps])
        return top, total, [p.astype(BF16) for p in ps]

    def scores_of(keys, queries, b):
        return lax.dot_general(keys, queries, NT, preferred_element_type=F32) * SCALE + b

    def tile(g):
        return pl.ds(pl.multiple_of(g * T, T), T)

    def rows_of(ref, *where):
        return ref[where].reshape(-1, HEAD)

    def context(h):
        @pl.when(before[1])
        def _():
            for u in range(2):
                send_k(h, u).wait_recv()
                send_v(h, u).wait_recv()

        v1t[h] = rows_of(v1, h).T

    def widest(i):
        h = lax.div(i, 2)

        @pl.when(before[1] & after[3])
        def _():
            send_q3(i).wait_recv()
            for s in range(2):
                t = 2 * i + s
                g = t - h * G
                q = rows_of(q3, t)
                top, total, (p4, p3) = softmax_of([
                    scores_of(rows_of(k1, h, g), q, bias3[0]),
                    scores_of(rows_of(k0, h, g), q, bias3[1])])
                o = (jnp.dot(v1t[h, :, tile(g)], p4, preferred_element_type=F32)
                     + jnp.dot(v0t[h, :, tile(g)], p3, preferred_element_type=F32))
                o3[t] = (o * (1.0 / total)).astype(BF16)
                l3[t] = top + jnp.log2(total)
            for copy in send_o3(i):
                copy.start()

    def extra(i):
        h = lax.div(i, 2)

        @pl.when((c == 1) & after[2])
        def _():
            send_qx(i).wait_recv()
            for s in range(2):
                t = 2 * i + s
                g = t - h * G
                top, total, (p3,) = softmax_of([scores_of(rows_of(k1, h, g), rows_of(qx, t), bias2[...])])
                o = jnp.dot(v1t[h, :, tile(g)], p3, preferred_element_type=F32)
                ox[t] = (o * (1.0 / total)).astype(BF16)
                lx[t] = top + jnp.log2(total)
            for copy in send_ox(i):
                copy.start()

    def local(h):
        @pl.loop(0, G)
        def _(g):
            q = rows_of(q0, h * G + g)
            top, total, (p_prev, p_own) = softmax_of([
                scores_of(rows_of(k1, h), q, bias[g, 0]), scores_of(rows_of(k0, h), q, bias[g, 1])])
            o = (jnp.dot(v1t[h], p_prev, preferred_element_type=F32)
                 + jnp.dot(v0t[h], p_own, preferred_element_type=F32))
            loc_o[h * G + g] = o
            loc_m[h * G + g] = top
            loc_l[h * G + g] = total

    def answer(i):
        @pl.when(before[1] & after[1])
        def _():
            @pl.when(before[2])
            def _():
                for copy in send_o3(i):
                    copy.wait_recv()

            h = lax.div(i, 2)
            for s in range(2):
                t = 2 * i + s
                g = t - h * G
                top, total, (p2,) = softmax_of([scores_of(rows_of(k1, h, g), rows_of(q1, t), bias2[...])])
                o = jnp.dot(v1t[h, :, tile(g)], p2, preferred_element_type=F32)
                lse = l3_in[t]
                peak = jnp.maximum(top, lse)
                here = jnp.exp2(top - peak)
                there = jnp.exp2(lse - peak)
                whole = total * here + there
                o1[t] = (o * (here / whole) + o3_in[t].astype(F32) * (there / whole)).astype(BF16)
                l1[t] = peak + jnp.log2(whole)
            for copy in send_o1(i):
                copy.start()

    def i32(i):
        return jnp.int32(i)

    def wide(i):
        widest(i32(i))
        extra(i32(i))

    with jax.named_scope("wide03"):
        context(0)
        wide(0)
        wide(1)
        context(1)
        wide(2)
        pass_on(half)
        wide(3)
        pass_on(half + 1)
    with jax.named_scope("local0"):
        local(0)
        pass_on(half + 2)
        answer(i32(0))
    with jax.named_scope("local1"):
        local(1)
        pass_on(half + 3)
        answer(i32(1))
        answer(i32(2))
    with jax.named_scope("wide45"):
        context(2)
        wide(4)
        answer(i32(3))
        local(2)
        wide(5)
    with jax.named_scope("wide67"):
        context(3)
        wide(6)
        local(3)
        wide(7)

    def row_block(b):
        return slice(b * T, (b + 1) * T)

    def term(u, h, b):
        start = pl.multiple_of(u * width + h * HEAD, HEAD)
        return jnp.dot(mixed[u, h, row_block(b), :], wo_v[pl.ds(start, HEAD), :], preferred_element_type=F32)

    def finish(h):
        with jax.named_scope(f"head{h}"):
            @pl.when(before[2])
            def _():
                for i in (2 * h, 2 * h + 1):
                    for copy in send_o1(i):
                        copy.wait_recv()

            for g in range(G):
                t = h * G + g
                top, lse = loc_m[t], l1_in[t]
                peak = jnp.maximum(top, lse)
                here = jnp.exp2(top - peak)
                there = jnp.exp2(lse - peak)
                whole = loc_l[t] * here + there
                o = loc_o[t] * (here / whole) + o1_in[t].astype(F32) * (there / whole)
                mix_t[h, :, g * T:(g + 1) * T] = o.astype(BF16)
            mixed[tp, h] = lax.dot_general(perm_out[...], mix_t[h], NT, preferred_element_type=F32).astype(BF16)
            send_mixed(h).start()
        with jax.named_scope(f"acc{h}"):
            for b in range(G):
                y = term(tp, h, b)
                acc[row_block(b)] = y if h == 0 else acc[row_block(b)] + y
            if h < heads - 1:
                send_mixed(h).wait_recv()
                for b in range(G):
                    acc[row_block(b)] += term(1 - tp, h, b)

    load(4).wait()
    with jax.named_scope("final"):
        finish(0)
    with jax.named_scope("o1b"):
        for i in (half, half + 1):
            answer(jnp.int32(i))
    with jax.named_scope("finalb"):
        finish(1)
    with jax.named_scope("o1c"):
        for i in range(half + 2, chunks):
            answer(jnp.int32(i))
    with jax.named_scope("finalc"):
        for h in range(2, heads):
            finish(h)

    with jax.named_scope("out"):
        send_mixed(heads - 1).wait_recv()
        for b in range(G):
            out_v[row_block(b)] = (acc[row_block(b)] + term(1 - tp, heads - 1, b)).astype(BF16)
            send_out(b).start()

    with jax.named_scope("drain"):
        send_tokens().wait_send()

        @pl.when(after[1])
        def _():
            for h in range(heads):
                for u in range(2):
                    send_k(h, u).wait_send()
                    send_v(h, u).wait_send()

        @pl.loop(0, chunks)
        def _(i):
            @pl.when(before[2])
            def _():
                send_q1(i).wait_send()

            @pl.when(before[3] & after[1])
            def _():
                send_q3(i).wait_send()

            @pl.when((c == 2) & after[1])
            def _():
                send_qx(i).wait_send()

            @pl.when((c == 1) & after[2])
            def _():
                for copy in send_ox(i):
                    copy.wait_send()

            @pl.when(before[1] & after[3])
            def _():
                for copy in send_o3(i):
                    copy.wait_send()

            @pl.when(before[1] & after[1])
            def _():
                for copy in send_o1(i):
                    copy.wait_send()

        for h in range(heads):
            send_mixed(h).wait_send()
        for b in range(G):
            send_out(b).wait()


def body(tokens, query_weight, key_weight, value_weight, output_weight):
    n = lax.axis_size("sp")
    half_rows, depth = tokens.shape
    width = query_weight.shape[1]
    heads = width // HEAD
    tiles, chunks = heads * G, 2 * heads
    features = output_weight.shape[1]
    assert 2 * half_rows == ROWS and FAR_DILATION == MIDDLE_DILATION**2 and heads % 2 == 0
    assert output_weight.shape[0] == 2 * width
    vmem = pltpu.VMEM
    dma = pltpu.SemaphoreType.DMA
    split = (tiles, 2, T // 2, HEAD)
    by_head = (heads, G, 2, T // 2, HEAD)
    turned = (heads, HEAD, ROWS)
    square = (tiles, T, HEAD)
    stat = (tiles, 1, T)
    scratch = [
        vmem((2, half_rows, depth), BF16), vmem((2, half_rows, depth), BF16),
        vmem((depth, width), BF16), vmem((depth, width), BF16), vmem((depth, width), BF16),
        vmem((2 * width, features), BF16), vmem((ROWS, features), BF16), vmem((ROWS, features), F32),
        vmem((2, half_rows, HEAD), F32), vmem((2, half_rows, HEAD), F32),
        vmem((G, 2, ROWS, T), F32), vmem((T, T), F32), vmem((2, T, T), F32),
        vmem((half_rows, half_rows), BF16), vmem((ROWS, ROWS), BF16),
        vmem(split, BF16),
        vmem(by_head, BF16), vmem(by_head, BF16), vmem(by_head, BF16), vmem(by_head, BF16),
        vmem(turned, BF16), vmem(turned, BF16),
        vmem(split, BF16), vmem(split, BF16), vmem(split, BF16), vmem(square, BF16), vmem(stat, F32),
        vmem(square, BF16), vmem(stat, F32), vmem(square, BF16), vmem(stat, F32),
        vmem(square, BF16), vmem(stat, F32), vmem(square, BF16), vmem(stat, F32),
        vmem(square, F32), vmem(stat, F32), vmem(stat, F32),
        vmem(turned, BF16), vmem((2, heads, ROWS, HEAD), BF16),
        dma((5,)), dma((2, 1)), dma((2, chunks)), dma((2, chunks)), dma((2, chunks)), dma((2, chunks)),
        dma((2, chunks)), dma((2, chunks)), dma((2, chunks)), dma((2, chunks)), dma((2, chunks)), dma((2, chunks)), dma((2, heads)), dma((G,)),
    ]
    hbm = pl.BlockSpec(memory_space=pltpu.HBM)
    return pl.pallas_call(
        functools.partial(kernel, n),
        out_shape=jax.ShapeDtypeStruct((ROWS, features), BF16),
        in_specs=[hbm] * 5,
        out_specs=pl.BlockSpec(memory_space=pl.ANY),
        scratch_shapes=scratch,
        compiler_params=pltpu.CompilerParams(
            collective_id=0, has_side_effects=True, vmem_limit_bytes=VMEM_LIMIT),
        name="attention",
    )(tokens, query_weight, key_weight, value_weight, output_weight)


def solution(mesh):
    in_specs = (
        P(("grp", "sp", "tp"), None),
        P(None, "tp"),
        P(None, "tp"),
        P(None, "tp"),
        P(None, "tp"),
    )
    out_specs = P(("grp", "sp"), "tp")
    return jax.shard_map(body, mesh=mesh, in_specs=in_specs, out_specs=out_specs, check_vma=False)
```

```python
import functools
import math

import jax
import jax.numpy as jnp
from jax import lax
from jax.experimental import pallas as pl
from jax.experimental.pallas import tpu as pltpu
from jax.sharding import PartitionSpec as P

HEAD = 128
REACH_STEPS = 128
MIDDLE_DILATION = 4
FAR_DILATION = 16
THETA_BASE = 500000.0

MESH = pl.DeviceIdType.MESH
F32 = jnp.float32
BF16 = jnp.bfloat16
G = MIDDLE_DILATION
T = REACH_STEPS
ROWS = G * T
NEG = -1e30
VMEM_LIMIT = 55_000_000
SCALE = HEAD**-0.5 * math.log2(math.e)
NT = (((1,), (1,)), ((), ()))


def iota(shape, dim):
    return lax.broadcasted_iota(jnp.int32, shape, dim)


def sin_cos(x):
    n = jnp.floor(x * (2.0 / math.pi) + 0.5)
    r = ((x - n * 1.5703125) - n * 4.837512969970703125e-4) - n * 7.549789954891882e-8
    z = r * r
    s = r + r * z * ((-1.9515295891e-4 * z + 8.3321608736e-3) * z - 1.6666654611e-1)
    c = 1.0 - 0.5 * z + z * z * ((2.443315711809948e-5 * z - 1.388731625493765e-3) * z + 4.166664568298827e-2)
    k = n.astype(jnp.int32) & 3
    odd = (k & 1) == 1
    sine = jnp.where(odd, c, s)
    cosine = jnp.where(odd, s, c)
    sine = jnp.where((k & 2) == 2, -sine, sine)
    cosine = jnp.where(((k + 1) & 2) == 2, -cosine, cosine)
    return sine, cosine


def kernel(n, tokens, wq, wk, wv, wo, out,
           x_nat, x, wq_v, wk_v, wv_v, wo_v, out_v, acc,
           rope_c, rope_s, bias, bias2, bias3, perm_in, perm_out,
           q0, k0, v0, k1, v1, v0t, v1t, q1, q3, qx, ox, lx,
           o3, l3, o3_in, l3_in, o1, l1, o1_in, l1_in,
           loc_o, loc_m, loc_l, mix_t, mixed,
           load_sem, tok_sem, k_sem, v_sem, q1_sem, q3_sem,
           o3_sem, l3_sem, o1_sem, l1_sem, qx_sem, ox_sem, mix_sem, out_sem):
    c = lax.axis_index("sp")
    tp = lax.axis_index("tp")
    heads = k0.shape[0]
    width = heads * HEAD
    chunks = 2 * heads
    pairs = heads // 2
    half_rows = ROWS // 2
    piece = T // 2
    partner = {"tp": 1 - tp}

    before = [None, c >= 1, c >= 2, c >= 3]
    after = [None, c + 1 < n, c + 2 < n, c + 3 < n]

    def at(distance):
        return {"sp": jnp.clip(c + distance, 0, n - 1)}

    def load(i):
        src, dst = ((tokens, x_nat.at[tp]), (wk, wk_v), (wv, wv_v), (wq, wq_v), (wo, wo_v))[i]
        return pltpu.make_async_copy(src, dst, load_sem.at[i])

    for i in range(5):
        load(i).start()

    barrier = pltpu.get_barrier_semaphore()

    def greet(device):
        pl.semaphore_signal(barrier, inc=1, device_id=device, device_id_type=MESH)

    greet(partner)
    pl.when(before[1])(functools.partial(greet, at(-1)))
    pl.when(before[3])(functools.partial(greet, at(-2)))
    pl.when(before[1] & after[1])(functools.partial(greet, at(1)))
    pl.when(before[1] & after[2])(functools.partial(greet, at(2)))

    def remote(src, dst, sems, i, device):
        return pltpu.make_async_remote_copy(
            src_ref=src, dst_ref=dst, send_sem=sems.at[0, i], recv_sem=sems.at[1, i],
            device_id=device, device_id_type=MESH)

    def send_tokens():
        return remote(tokens, x_nat.at[tp], tok_sem, 0, partner)

    def send_k(h, u):
        return remote(k0.at[h, :, u], k1.at[h, :, u], k_sem, 2 * h + u, at(1))

    def send_v(h, u):
        return remote(v0.at[h, :, u], v1.at[h, :, u], v_sem, 2 * h + u, at(1))

    def chunk(ref, i):
        return ref.at[pl.ds(2 * i, 2)]

    def send_q1(i):
        return remote(chunk(q0, i), chunk(q1, i), q1_sem, i, at(-1))

    def send_q3(i):
        return remote(chunk(q1, i), chunk(q3, i), q3_sem, i, at(-2))

    def send_qx(i):
        return remote(chunk(q1, i), chunk(qx, i), qx_sem, i, at(-1))

    def send_ox(i):
        return tuple(
            pltpu.make_async_remote_copy(
                src_ref=chunk(src, i), dst_ref=chunk(dst, i), send_sem=ox_sem.at[k, i], recv_sem=sems.at[1, i],
                device_id=at(1), device_id_type=MESH)
            for k, (src, dst, sems) in enumerate(((ox, o3_in, o3_sem), (lx, l3_in, l3_sem))))

    def send_o3(i):
        return (remote(chunk(o3, i), chunk(o3_in, i), o3_sem, i, at(2)),
                remote(chunk(l3, i), chunk(l3_in, i), l3_sem, i, at(2)))

    def send_o1(i):
        return (remote(chunk(o1, i), chunk(o1_in, i), o1_sem, i, at(1)),
                remote(chunk(l1, i), chunk(l1_in, i), l1_sem, i, at(1)))

    def send_mixed(h):
        return remote(mixed.at[tp, h], mixed.at[tp, h], mix_sem, h, partner)

    def send_out(b):
        rows = pl.ds(b * T, T)
        return pltpu.make_async_copy(out_v.at[rows], out.at[rows], out_sem.at[b])

    with jax.named_scope("tables"):
        row = iota((half_rows, half_rows), 0)
        col = iota((half_rows, half_rows), 1)
        perm_in[...] = jnp.where(row == (col & (G - 1)) * piece + lax.shift_right_logical(col, 2), 1.0, 0.0).astype(BF16)

        lane = iota((T, HEAD), 1)
        index = lane & (HEAD // 2 - 1)
        inverse = jnp.ones((T, HEAD), F32)
        for bit in range(6):
            factor = THETA_BASE ** (-(2.0**bit) / (HEAD // 2))
            inverse = jnp.where((lax.shift_right_logical(index, bit) & 1) == 1, inverse * factor, inverse)

        @pl.loop(0, 4)
        def _(i):
            u = lax.shift_right_logical(i, 1)
            r = iota((T, HEAD), 0) + (i & 1) * T
            local = (r & (piece - 1)) * G + lax.shift_right_logical(r, 6)
            position = c * ROWS + u * half_rows + local
            sine, cosine = sin_cos(position.astype(F32) * inverse)
            rows = pl.ds(pl.multiple_of((i & 1) * T, T), T)
            rope_c[u, rows, :] = cosine
            rope_s[u, rows, :] = jnp.where(lane < HEAD // 2, -sine, sine)

    def permuted(u):
        x[u] = jnp.dot(perm_in[...], x_nat[u], preferred_element_type=F32).astype(BF16)

    def columns(p):
        return slice(2 * p * HEAD, (2 * p + 2) * HEAD)

    def rotated(y, u):
        return (y * rope_c[u] + pltpu.roll(y, HEAD // 2, 1) * rope_s[u]).astype(BF16)

    def project(w, p, u):
        return jnp.dot(x[u], w[:, columns(p)], preferred_element_type=F32)

    def make_k(p, u):
        y = project(wk_v, p, u)
        for s in range(2):
            z = rotated(y[:, s * HEAD:(s + 1) * HEAD], u)
            for g in range(G):
                k0[2 * p + s, g, u] = z[g * piece:(g + 1) * piece]

    def make_v(p, u):
        y = project(wv_v, p, u).astype(BF16)
        for s in range(2):
            for g in range(G):
                v0[2 * p + s, g, u] = y[g * piece:(g + 1) * piece, s * HEAD:(s + 1) * HEAD]

    def forward(send, h, u):
        @pl.when(after[1])
        def _():
            send(h, u).start()

    with jax.named_scope("own_k"):
        load(0).wait()
        permuted(tp)
        load(1).wait()
        make_k(0, tp)

    with jax.named_scope("barrier"):
        count = 1
        for exists in (after[1], before[2], before[1] & after[2], before[3]):
            count = count + exists.astype(jnp.int32)
        pl.semaphore_wait(barrier, count)
        send_tokens().start()

    with jax.named_scope("own_kv"):
        forward(send_k, 0, tp)
        load(2).wait()
        make_v(0, tp)
        forward(send_v, 0, tp)

    @pl.when(c < 1)
    def _():
        k1[...] = jnp.zeros_like(k1)
        v1[...] = jnp.zeros_like(v1)

    @pl.when(c < 2)
    def _():
        o3_in[...] = jnp.zeros_like(o3_in)
        l3_in[...] = jnp.full_like(l3_in, NEG)
        o1_in[...] = jnp.zeros_like(o1_in)
        l1_in[...] = jnp.full_like(l1_in, NEG)

    def make_q(p):
        y = jnp.dot(x[...].reshape(ROWS, x.shape[2]), wq_v[:, columns(p)], preferred_element_type=F32)
        for s in range(2):
            for u in range(2):
                z = rotated(y[u * half_rows:(u + 1) * half_rows, s * HEAD:(s + 1) * HEAD], u)
                for g in range(G):
                    q0[(2 * p + s) * G + g, u] = z[g * piece:(g + 1) * piece]

    half = chunks // 2

    def ask(p):
        @pl.when(before[2])
        def _():
            for i in range(p * half, (p + 1) * half):
                send_q1(i).start()

    with jax.named_scope("own_kv1"):
        make_k(1, tp)

    with jax.named_scope("tokwait"):
        send_tokens().wait_recv()

    with jax.named_scope("other_kv0"):
        permuted(1 - tp)
        make_k(0, 1 - tp)
        forward(send_k, 0, 1 - tp)
        make_v(0, 1 - tp)
        forward(send_v, 0, 1 - tp)
        for u in (tp, 1 - tp):
            forward(send_k, 1, u)
            forward(send_v, 1, u)

    with jax.named_scope("q0"):
        load(3).wait()
        make_q(0)
        ask(0)

    with jax.named_scope("kv1"):
        make_v(1, tp)
        make_k(1, 1 - tp)
        make_v(1, 1 - tp)
        for h in (2, 3):
            for u in (tp, 1 - tp):
                forward(send_k, h, u)
                forward(send_v, h, u)

    with jax.named_scope("q1"):
        make_q(1)

    with jax.named_scope("bias"):
        jk = iota((T, T), 0)
        jq = iota((T, T), 1)
        same = ((jq - jk) & (FAR_DILATION // MIDDLE_DILATION - 1)) == 0
        far = jnp.where(same, 0.0, NEG)
        bias2[...] = far
        bias3[0] = jnp.where(same & (jk >= jq), 0.0, NEG) + jnp.where(before[1], 0.0, NEG)
        bias3[1] = far

        @pl.loop(0, 2 * G)
        def _(b):
            which = lax.shift_right_logical(b, 2)
            gk = b & (G - 1)

            @pl.loop(0, G)
            def _(gq):
                k_pos = (iota((T, T), 0) - T * (1 - which)) * G + gk
                d = iota((T, T), 1) * G + gq - k_pos
                ok = d >= 0
                near = jnp.where(ok & (d <= REACH_STEPS), 1, 0)
                mid = jnp.where(ok & (d <= REACH_STEPS * MIDDLE_DILATION) & ((d & (MIDDLE_DILATION - 1)) == 0), 1, 0)
                wide = jnp.where(ok & (d <= REACH_STEPS * FAR_DILATION) & ((d & (FAR_DILATION - 1)) == 0), 1, 0)
                times = near + mid + wide
                value = jnp.where(times == 3, math.log2(3.0), jnp.where(times == 2, 1.0, jnp.where(times == 1, 0.0, NEG)))
                value = value + jnp.where((which == 1) | before[1], 0.0, NEG)
                bias[gq, which, pl.ds(pl.multiple_of(gk * T, T), T), :] = value

    def pass_on(i):
        @pl.when(before[1] & after[1])
        def _():
            send_q1(i).wait_recv()

            @pl.when(before[3])
            def _():
                send_q3(i).start()

            @pl.when(c == 2)
            def _():
                send_qx(i).start()

    with jax.named_scope("fwdq"):
        @pl.loop(0, half)
        def _(i):
            pass_on(i)

        ask(1)

        @pl.loop(0, G)
        def _(g):
            t = g * T + iota((T, ROWS), 0)
            s = iota((T, ROWS), 1)
            perm_out[pl.ds(pl.multiple_of(g * T, T), T), :] = jnp.where(
                s == (t & (G - 1)) * T + lax.shift_right_logical(t, 2), 1.0, 0.0).astype(BF16)

        for h in range(heads):
            v0t[h] = v0[h].reshape(ROWS, HEAD).T

    def softmax_of(scores):
        top = functools.reduce(jnp.maximum, [jnp.max(s, axis=0, keepdims=True) for s in scores])
        ps = [jnp.exp2(s - top) for s in scores]
        total = functools.reduce(jnp.add, [jnp.sum(p, axis=0, keepdims=True) for p in ps])
        return top, total, [p.astype(BF16) for p in ps]

    def scores_of(keys, queries, b):
        return lax.dot_general(keys, queries, NT, preferred_element_type=F32) * SCALE + b

    def tile(g):
        return pl.ds(pl.multiple_of(g * T, T), T)

    def rows_of(ref, *where):
        return ref[where].reshape(-1, HEAD)

    def context(h):
        @pl.when(before[1])
        def _():
            for u in range(2):
                send_k(h, u).wait_recv()
                send_v(h, u).wait_recv()

        v1t[h] = rows_of(v1, h).T

    def widest(i):
        h = lax.div(i, 2)

        @pl.when(before[1] & after[3])
        def _():
            send_q3(i).wait_recv()
            for s in range(2):
                t = 2 * i + s
                g = t - h * G
                q = rows_of(q3, t)
                top, total, (p4, p3) = softmax_of([
                    scores_of(rows_of(k1, h, g), q, bias3[0]),
                    scores_of(rows_of(k0, h, g), q, bias3[1])])
                o = (jnp.dot(v1t[h, :, tile(g)], p4, preferred_element_type=F32)
                     + jnp.dot(v0t[h, :, tile(g)], p3, preferred_element_type=F32))
                o3[t] = (o * (1.0 / total)).astype(BF16)
                l3[t] = top + jnp.log2(total)
            for copy in send_o3(i):
                copy.start()

    def extra(i):
        h = lax.div(i, 2)

        @pl.when((c == 1) & after[2])
        def _():
            send_qx(i).wait_recv()
            for s in range(2):
                t = 2 * i + s
                g = t - h * G
                top, total, (p3,) = softmax_of([scores_of(rows_of(k1, h, g), rows_of(qx, t), bias2[...])])
                o = jnp.dot(v1t[h, :, tile(g)], p3, preferred_element_type=F32)
                ox[t] = (o * (1.0 / total)).astype(BF16)
                lx[t] = top + jnp.log2(total)
            for copy in send_ox(i):
                copy.start()

    def local(h):
        @pl.loop(0, G)
        def _(g):
            q = rows_of(q0, h * G + g)
            top, total, (p_prev, p_own) = softmax_of([
                scores_of(rows_of(k1, h), q, bias[g, 0]), scores_of(rows_of(k0, h), q, bias[g, 1])])
            o = (jnp.dot(v1t[h], p_prev, preferred_element_type=F32)
                 + jnp.dot(v0t[h], p_own, preferred_element_type=F32))
            loc_o[h * G + g] = o
            loc_m[h * G + g] = top
            loc_l[h * G + g] = total

    def answer(i):
        @pl.when(before[1] & after[1])
        def _():
            @pl.when(before[2])
            def _():
                for copy in send_o3(i):
                    copy.wait_recv()

            h = lax.div(i, 2)
            for s in range(2):
                t = 2 * i + s
                g = t - h * G
                top, total, (p2,) = softmax_of([scores_of(rows_of(k1, h, g), rows_of(q1, t), bias2[...])])
                o = jnp.dot(v1t[h, :, tile(g)], p2, preferred_element_type=F32)
                lse = l3_in[t]
                peak = jnp.maximum(top, lse)
                here = jnp.exp2(top - peak)
                there = jnp.exp2(lse - peak)
                whole = total * here + there
                o1[t] = (o * (here / whole) + o3_in[t].astype(F32) * (there / whole)).astype(BF16)
                l1[t] = peak + jnp.log2(whole)
            for copy in send_o1(i):
                copy.start()

    def i32(i):
        return jnp.int32(i)

    def wide(i):
        widest(i32(i))
        extra(i32(i))

    def early(i):
        pl.when(after[2])(functools.partial(pass_on, i))

    with jax.named_scope("wide03"):
        context(0)
        wide(0)
        wide(1)
        context(1)
        wide(2)
        early(half)
        wide(3)
        early(half + 1)
    with jax.named_scope("local0"):
        local(0)
        early(half + 2)
        answer(i32(0))
    with jax.named_scope("local1"):
        local(1)
        early(half + 3)
        answer(i32(1))
        answer(i32(2))

        @pl.when(c + 2 == n)
        def _():
            for i in range(half, chunks):
                pass_on(i)

    with jax.named_scope("wide45"):
        context(2)
        wide(4)
        answer(i32(3))
        local(2)
        wide(5)
    with jax.named_scope("wide67"):
        context(3)
        wide(6)
        local(3)
        wide(7)

    def row_block(b):
        return slice(b * T, (b + 1) * T)

    def term(u, h, b):
        start = pl.multiple_of(u * width + h * HEAD, HEAD)
        return jnp.dot(mixed[u, h, row_block(b), :], wo_v[pl.ds(start, HEAD), :], preferred_element_type=F32)

    def finish(h):
        with jax.named_scope(f"head{h}"):
            @pl.when(before[2])
            def _():
                for i in (2 * h, 2 * h + 1):
                    for copy in send_o1(i):
                        copy.wait_recv()

            for g in range(G):
                t = h * G + g
                top, lse = loc_m[t], l1_in[t]
                peak = jnp.maximum(top, lse)
                here = jnp.exp2(top - peak)
                there = jnp.exp2(lse - peak)
                whole = loc_l[t] * here + there
                o = loc_o[t] * (here / whole) + o1_in[t].astype(F32) * (there / whole)
                mix_t[h, :, g * T:(g + 1) * T] = o.astype(BF16)
            mixed[tp, h] = lax.dot_general(perm_out[...], mix_t[h], NT, preferred_element_type=F32).astype(BF16)
            send_mixed(h).start()
        with jax.named_scope(f"acc{h}"):
            for b in range(G):
                y = term(tp, h, b)
                acc[row_block(b)] = y if h == 0 else acc[row_block(b)] + y
            if h < heads - 1:
                send_mixed(h).wait_recv()
                for b in range(G):
                    acc[row_block(b)] += term(1 - tp, h, b)

    load(4).wait()
    with jax.named_scope("final"):
        finish(0)
    with jax.named_scope("o1b"):
        for i in (half, half + 1):
            answer(jnp.int32(i))
    with jax.named_scope("finalb"):
        finish(1)
    with jax.named_scope("o1c"):
        for i in range(half + 2, chunks):
            answer(jnp.int32(i))
    with jax.named_scope("finalc"):
        for h in range(2, heads):
            finish(h)

    with jax.named_scope("out"):
        send_mixed(heads - 1).wait_recv()
        for b in range(G):
            out_v[row_block(b)] = (acc[row_block(b)] + term(1 - tp, heads - 1, b)).astype(BF16)
            send_out(b).start()

    with jax.named_scope("drain"):
        send_tokens().wait_send()

        @pl.when(after[1])
        def _():
            for h in range(heads):
                for u in range(2):
                    send_k(h, u).wait_send()
                    send_v(h, u).wait_send()

        @pl.loop(0, chunks)
        def _(i):
            @pl.when(before[2])
            def _():
                send_q1(i).wait_send()

            @pl.when(before[3] & after[1])
            def _():
                send_q3(i).wait_send()

            @pl.when((c == 2) & after[1])
            def _():
                send_qx(i).wait_send()

            @pl.when((c == 1) & after[2])
            def _():
                for copy in send_ox(i):
                    copy.wait_send()

            @pl.when(before[1] & after[3])
            def _():
                for copy in send_o3(i):
                    copy.wait_send()

            @pl.when(before[1] & after[1])
            def _():
                for copy in send_o1(i):
                    copy.wait_send()

        for h in range(heads):
            send_mixed(h).wait_send()
        for b in range(G):
            send_out(b).wait()


def body(tokens, query_weight, key_weight, value_weight, output_weight):
    n = lax.axis_size("sp")
    half_rows, depth = tokens.shape
    width = query_weight.shape[1]
    heads = width // HEAD
    tiles, chunks = heads * G, 2 * heads
    features = output_weight.shape[1]
    assert 2 * half_rows == ROWS and FAR_DILATION == MIDDLE_DILATION**2 and heads % 2 == 0
    assert output_weight.shape[0] == 2 * width
    vmem = pltpu.VMEM
    dma = pltpu.SemaphoreType.DMA
    split = (tiles, 2, T // 2, HEAD)
    by_head = (heads, G, 2, T // 2, HEAD)
    turned = (heads, HEAD, ROWS)
    square = (tiles, T, HEAD)
    stat = (tiles, 1, T)
    scratch = [
        vmem((2, half_rows, depth), BF16), vmem((2, half_rows, depth), BF16),
        vmem((depth, width), BF16), vmem((depth, width), BF16), vmem((depth, width), BF16),
        vmem((2 * width, features), BF16), vmem((ROWS, features), BF16), vmem((ROWS, features), F32),
        vmem((2, half_rows, HEAD), F32), vmem((2, half_rows, HEAD), F32),
        vmem((G, 2, ROWS, T), F32), vmem((T, T), F32), vmem((2, T, T), F32),
        vmem((half_rows, half_rows), BF16), vmem((ROWS, ROWS), BF16),
        vmem(split, BF16),
        vmem(by_head, BF16), vmem(by_head, BF16), vmem(by_head, BF16), vmem(by_head, BF16),
        vmem(turned, BF16), vmem(turned, BF16),
        vmem(split, BF16), vmem(split, BF16), vmem(split, BF16), vmem(square, BF16), vmem(stat, F32),
        vmem(square, BF16), vmem(stat, F32), vmem(square, BF16), vmem(stat, F32),
        vmem(square, BF16), vmem(stat, F32), vmem(square, BF16), vmem(stat, F32),
        vmem(square, F32), vmem(stat, F32), vmem(stat, F32),
        vmem(turned, BF16), vmem((2, heads, ROWS, HEAD), BF16),
        dma((5,)), dma((2, 1)), dma((2, chunks)), dma((2, chunks)), dma((2, chunks)), dma((2, chunks)),
        dma((2, chunks)), dma((2, chunks)), dma((2, chunks)), dma((2, chunks)), dma((2, chunks)), dma((2, chunks)), dma((2, heads)), dma((G,)),
    ]
    hbm = pl.BlockSpec(memory_space=pltpu.HBM)
    return pl.pallas_call(
        functools.partial(kernel, n),
        out_shape=jax.ShapeDtypeStruct((ROWS, features), BF16),
        in_specs=[hbm] * 5,
        out_specs=pl.BlockSpec(memory_space=pl.ANY),
        scratch_shapes=scratch,
        compiler_params=pltpu.CompilerParams(
            collective_id=0, has_side_effects=True, vmem_limit_bytes=VMEM_LIMIT),
        name="attention",
    )(tokens, query_weight, key_weight, value_weight, output_weight)


def solution(mesh):
    in_specs = (
        P(("grp", "sp", "tp"), None),
        P(None, "tp"),
        P(None, "tp"),
        P(None, "tp"),
        P(None, "tp"),
    )
    out_specs = P(("grp", "sp"), "tp")
    return jax.shard_map(body, mesh=mesh, in_specs=in_specs, out_specs=out_specs, check_vma=False)
```

```python
import functools
import math

import jax
import jax.numpy as jnp
from jax import lax
from jax.experimental import pallas as pl
from jax.experimental.pallas import tpu as pltpu
from jax.sharding import PartitionSpec as P

HEAD = 128
REACH_STEPS = 128
MIDDLE_DILATION = 4
FAR_DILATION = 16
THETA_BASE = 500000.0

MESH = pl.DeviceIdType.MESH
F32 = jnp.float32
BF16 = jnp.bfloat16
G = MIDDLE_DILATION
T = REACH_STEPS
ROWS = G * T
NEG = -1e30
VMEM_LIMIT = 55_000_000
SCALE = HEAD**-0.5 * math.log2(math.e)
NT = (((1,), (1,)), ((), ()))


def iota(shape, dim):
    return lax.broadcasted_iota(jnp.int32, shape, dim)


def sin_cos(x):
    n = jnp.floor(x * (2.0 / math.pi) + 0.5)
    r = ((x - n * 1.5703125) - n * 4.837512969970703125e-4) - n * 7.549789954891882e-8
    z = r * r
    s = r + r * z * ((-1.9515295891e-4 * z + 8.3321608736e-3) * z - 1.6666654611e-1)
    c = 1.0 - 0.5 * z + z * z * ((2.443315711809948e-5 * z - 1.388731625493765e-3) * z + 4.166664568298827e-2)
    k = n.astype(jnp.int32) & 3
    odd = (k & 1) == 1
    sine = jnp.where(odd, c, s)
    cosine = jnp.where(odd, s, c)
    sine = jnp.where((k & 2) == 2, -sine, sine)
    cosine = jnp.where(((k + 1) & 2) == 2, -cosine, cosine)
    return sine, cosine


def kernel(n, tokens, wq, wk, wv, wo, out,
           x_nat, x, wq_v, wk_v, wv_v, wo_v, out_v, acc,
           rope_c, rope_s, bias, bias2, bias3, perm_in, perm_out,
           q0, k0, v0, k1, v1, v0t, v1t, q1, q3, qx, ox, lx,
           o3, l3, o3_in, l3_in, o1, l1, o1_in, l1_in,
           loc_o, loc_m, loc_l, mix_t, mixed,
           load_sem, tok_sem, k_sem, v_sem, q1_sem, q3_sem,
           o3_sem, l3_sem, o1_sem, l1_sem, qx_sem, ox_sem, mix_sem, out_sem):
    c = lax.axis_index("sp")
    tp = lax.axis_index("tp")
    heads = k0.shape[0]
    width = heads * HEAD
    chunks = 2 * heads
    pairs = heads // 2
    half_rows = ROWS // 2
    piece = T // 2
    partner = {"tp": 1 - tp}

    before = [None, c >= 1, c >= 2, c >= 3]
    after = [None, c + 1 < n, c + 2 < n, c + 3 < n]

    def at(distance):
        return {"sp": jnp.clip(c + distance, 0, n - 1)}

    def load(i):
        src, dst = ((tokens, x_nat.at[tp]), (wk, wk_v), (wv, wv_v), (wq, wq_v), (wo, wo_v))[i]
        return pltpu.make_async_copy(src, dst, load_sem.at[i])

    for i in range(2):
        load(i).start()

    barrier = pltpu.get_barrier_semaphore()

    def greet(device):
        pl.semaphore_signal(barrier, inc=1, device_id=device, device_id_type=MESH)

    greet(partner)
    pl.when(before[1])(functools.partial(greet, at(-1)))
    pl.when(before[3])(functools.partial(greet, at(-2)))
    pl.when(before[1] & after[1])(functools.partial(greet, at(1)))
    pl.when(before[1] & after[2])(functools.partial(greet, at(2)))

    def remote(src, dst, sems, i, device):
        return pltpu.make_async_remote_copy(
            src_ref=src, dst_ref=dst, send_sem=sems.at[0, i], recv_sem=sems.at[1, i],
            device_id=device, device_id_type=MESH)

    def send_tokens():
        return remote(tokens, x_nat.at[tp], tok_sem, 0, partner)

    def send_k(h, u):
        return remote(k0.at[h, :, u], k1.at[h, :, u], k_sem, 2 * h + u, at(1))

    def send_v(h, u):
        return remote(v0.at[h, :, u], v1.at[h, :, u], v_sem, 2 * h + u, at(1))

    def chunk(ref, i):
        return ref.at[pl.ds(2 * i, 2)]

    def send_q1(i):
        return remote(chunk(q0, i), chunk(q1, i), q1_sem, i, at(-1))

    def send_q3(i):
        return remote(chunk(q1, i), chunk(q3, i), q3_sem, i, at(-2))

    def send_qx(i):
        return remote(chunk(q1, i), chunk(qx, i), qx_sem, i, at(-1))

    def send_ox(i):
        return tuple(
            pltpu.make_async_remote_copy(
                src_ref=chunk(src, i), dst_ref=chunk(dst, i), send_sem=ox_sem.at[k, i], recv_sem=sems.at[1, i],
                device_id=at(1), device_id_type=MESH)
            for k, (src, dst, sems) in enumerate(((ox, o3_in, o3_sem), (lx, l3_in, l3_sem))))

    def send_o3(i):
        return (remote(chunk(o3, i), chunk(o3_in, i), o3_sem, i, at(2)),
                remote(chunk(l3, i), chunk(l3_in, i), l3_sem, i, at(2)))

    def send_o1(i):
        return (remote(chunk(o1, i), chunk(o1_in, i), o1_sem, i, at(1)),
                remote(chunk(l1, i), chunk(l1_in, i), l1_sem, i, at(1)))

    def send_mixed(h):
        return remote(mixed.at[tp, h], mixed.at[tp, h], mix_sem, h, partner)

    def send_out(b):
        rows = pl.ds(b * T, T)
        return pltpu.make_async_copy(out_v.at[rows], out.at[rows], out_sem.at[b])

    with jax.named_scope("tables"):
        row = iota((half_rows, half_rows), 0)
        col = iota((half_rows, half_rows), 1)
        perm_in[...] = jnp.where(row == (col & (G - 1)) * piece + lax.shift_right_logical(col, 2), 1.0, 0.0).astype(BF16)

        lane = iota((T, HEAD), 1)
        index = lane & (HEAD // 2 - 1)
        inverse = jnp.ones((T, HEAD), F32)
        for bit in range(6):
            factor = THETA_BASE ** (-(2.0**bit) / (HEAD // 2))
            inverse = jnp.where((lax.shift_right_logical(index, bit) & 1) == 1, inverse * factor, inverse)

        @pl.loop(0, 4)
        def _(i):
            u = lax.shift_right_logical(i, 1)
            r = iota((T, HEAD), 0) + (i & 1) * T
            local = (r & (piece - 1)) * G + lax.shift_right_logical(r, 6)
            position = c * ROWS + u * half_rows + local
            sine, cosine = sin_cos(position.astype(F32) * inverse)
            rows = pl.ds(pl.multiple_of((i & 1) * T, T), T)
            rope_c[u, rows, :] = cosine
            rope_s[u, rows, :] = jnp.where(lane < HEAD // 2, -sine, sine)

    def permuted(u):
        x[u] = jnp.dot(perm_in[...], x_nat[u], preferred_element_type=F32).astype(BF16)

    def columns(p):
        return slice(2 * p * HEAD, (2 * p + 2) * HEAD)

    def rotated(y, u):
        return (y * rope_c[u] + pltpu.roll(y, HEAD // 2, 1) * rope_s[u]).astype(BF16)

    def project(w, p, u):
        return jnp.dot(x[u], w[:, columns(p)], preferred_element_type=F32)

    def make_k(p, u):
        y = project(wk_v, p, u)
        for s in range(2):
            z = rotated(y[:, s * HEAD:(s + 1) * HEAD], u)
            for g in range(G):
                k0[2 * p + s, g, u] = z[g * piece:(g + 1) * piece]

    def make_v(p, u):
        y = project(wv_v, p, u).astype(BF16)
        for s in range(2):
            for g in range(G):
                v0[2 * p + s, g, u] = y[g * piece:(g + 1) * piece, s * HEAD:(s + 1) * HEAD]

    def forward(send, h, u):
        @pl.when(after[1])
        def _():
            send(h, u).start()

    with jax.named_scope("own_k"):
        load(0).wait()
        load(2).start()
        permuted(tp)
        load(1).wait()
        for i in (3, 4):
            load(i).start()
        make_k(0, tp)

    with jax.named_scope("barrier"):
        count = 1
        for exists in (after[1], before[2], before[1] & after[2], before[3]):
            count = count + exists.astype(jnp.int32)
        pl.semaphore_wait(barrier, count)
        send_tokens().start()

    with jax.named_scope("own_kv"):
        forward(send_k, 0, tp)
        load(2).wait()
        make_v(0, tp)
        forward(send_v, 0, tp)

    @pl.when(c < 1)
    def _():
        k1[...] = jnp.zeros_like(k1)
        v1[...] = jnp.zeros_like(v1)

    @pl.when(c < 2)
    def _():
        o3_in[...] = jnp.zeros_like(o3_in)
        l3_in[...] = jnp.full_like(l3_in, NEG)
        o1_in[...] = jnp.zeros_like(o1_in)
        l1_in[...] = jnp.full_like(l1_in, NEG)

    def make_q(p):
        y = jnp.dot(x[...].reshape(ROWS, x.shape[2]), wq_v[:, columns(p)], preferred_element_type=F32)
        for s in range(2):
            for u in range(2):
                z = rotated(y[u * half_rows:(u + 1) * half_rows, s * HEAD:(s + 1) * HEAD], u)
                for g in range(G):
                    q0[(2 * p + s) * G + g, u] = z[g * piece:(g + 1) * piece]

    half = chunks // 2

    def ask(p):
        @pl.when(before[2])
        def _():
            for i in range(p * half, (p + 1) * half):
                send_q1(i).start()

    with jax.named_scope("own_kv1"):
        make_k(1, tp)

    with jax.named_scope("tokwait"):
        send_tokens().wait_recv()

    with jax.named_scope("other_kv0"):
        permuted(1 - tp)
        make_k(0, 1 - tp)
        forward(send_k, 0, 1 - tp)
        make_v(0, 1 - tp)
        forward(send_v, 0, 1 - tp)
        for u in (tp, 1 - tp):
            forward(send_k, 1, u)
            forward(send_v, 1, u)

    with jax.named_scope("q0"):
        load(3).wait()
        make_q(0)
        ask(0)

    with jax.named_scope("kv1"):
        make_v(1, tp)
        make_k(1, 1 - tp)
        make_v(1, 1 - tp)
        for h in (2, 3):
            for u in (tp, 1 - tp):
                forward(send_k, h, u)
                forward(send_v, h, u)

    with jax.named_scope("q1"):
        make_q(1)

    with jax.named_scope("bias"):
        jk = iota((T, T), 0)
        jq = iota((T, T), 1)
        same = ((jq - jk) & (FAR_DILATION // MIDDLE_DILATION - 1)) == 0
        far = jnp.where(same, 0.0, NEG)
        bias2[...] = far
        bias3[0] = jnp.where(same & (jk >= jq), 0.0, NEG) + jnp.where(before[1], 0.0, NEG)
        bias3[1] = far

        @pl.loop(0, 2 * G)
        def _(b):
            which = lax.shift_right_logical(b, 2)
            gk = b & (G - 1)

            @pl.loop(0, G)
            def _(gq):
                k_pos = (iota((T, T), 0) - T * (1 - which)) * G + gk
                d = iota((T, T), 1) * G + gq - k_pos
                ok = d >= 0
                near = jnp.where(ok & (d <= REACH_STEPS), 1, 0)
                mid = jnp.where(ok & (d <= REACH_STEPS * MIDDLE_DILATION) & ((d & (MIDDLE_DILATION - 1)) == 0), 1, 0)
                wide = jnp.where(ok & (d <= REACH_STEPS * FAR_DILATION) & ((d & (FAR_DILATION - 1)) == 0), 1, 0)
                times = near + mid + wide
                value = jnp.where(times == 3, math.log2(3.0), jnp.where(times == 2, 1.0, jnp.where(times == 1, 0.0, NEG)))
                value = value + jnp.where((which == 1) | before[1], 0.0, NEG)
                bias[gq, which, pl.ds(pl.multiple_of(gk * T, T), T), :] = value

    def pass_on(i):
        @pl.when(before[1] & after[1])
        def _():
            send_q1(i).wait_recv()

            @pl.when(before[3])
            def _():
                send_q3(i).start()

            @pl.when(c == 2)
            def _():
                send_qx(i).start()

    with jax.named_scope("fwdq"):
        @pl.loop(0, half)
        def _(i):
            pass_on(i)

        ask(1)

        @pl.loop(0, G)
        def _(g):
            t = g * T + iota((T, ROWS), 0)
            s = iota((T, ROWS), 1)
            perm_out[pl.ds(pl.multiple_of(g * T, T), T), :] = jnp.where(
                s == (t & (G - 1)) * T + lax.shift_right_logical(t, 2), 1.0, 0.0).astype(BF16)

        for h in range(heads):
            v0t[h] = v0[h].reshape(ROWS, HEAD).T

    def softmax_of(scores):
        top = functools.reduce(jnp.maximum, [jnp.max(s, axis=0, keepdims=True) for s in scores])
        ps = [jnp.exp2(s - top) for s in scores]
        total = functools.reduce(jnp.add, [jnp.sum(p, axis=0, keepdims=True) for p in ps])
        return top, total, [p.astype(BF16) for p in ps]

    def scores_of(keys, queries, b):
        return lax.dot_general(keys, queries, NT, preferred_element_type=F32) * SCALE + b

    def tile(g):
        return pl.ds(pl.multiple_of(g * T, T), T)

    def rows_of(ref, *where):
        return ref[where].reshape(-1, HEAD)

    def context(h):
        @pl.when(before[1])
        def _():
            for u in range(2):
                send_k(h, u).wait_recv()
                send_v(h, u).wait_recv()

        v1t[h] = rows_of(v1, h).T

    def widest(i):
        h = lax.div(i, 2)

        @pl.when(before[1] & after[3])
        def _():
            send_q3(i).wait_recv()
            for s in range(2):
                t = 2 * i + s
                g = t - h * G
                q = rows_of(q3, t)
                top, total, (p4, p3) = softmax_of([
                    scores_of(rows_of(k1, h, g), q, bias3[0]),
                    scores_of(rows_of(k0, h, g), q, bias3[1])])
                o = (jnp.dot(v1t[h, :, tile(g)], p4, preferred_element_type=F32)
                     + jnp.dot(v0t[h, :, tile(g)], p3, preferred_element_type=F32))
                o3[t] = (o * (1.0 / total)).astype(BF16)
                l3[t] = top + jnp.log2(total)
            for copy in send_o3(i):
                copy.start()

    def extra(i):
        h = lax.div(i, 2)

        @pl.when((c == 1) & after[2])
        def _():
            send_qx(i).wait_recv()
            for s in range(2):
                t = 2 * i + s
                g = t - h * G
                top, total, (p3,) = softmax_of([scores_of(rows_of(k1, h, g), rows_of(qx, t), bias2[...])])
                o = jnp.dot(v1t[h, :, tile(g)], p3, preferred_element_type=F32)
                ox[t] = (o * (1.0 / total)).astype(BF16)
                lx[t] = top + jnp.log2(total)
            for copy in send_ox(i):
                copy.start()

    def local(h):
        @pl.loop(0, G)
        def _(g):
            q = rows_of(q0, h * G + g)
            top, total, (p_prev, p_own) = softmax_of([
                scores_of(rows_of(k1, h), q, bias[g, 0]), scores_of(rows_of(k0, h), q, bias[g, 1])])
            o = (jnp.dot(v1t[h], p_prev, preferred_element_type=F32)
                 + jnp.dot(v0t[h], p_own, preferred_element_type=F32))
            loc_o[h * G + g] = o
            loc_m[h * G + g] = top
            loc_l[h * G + g] = total

    def answer(i):
        @pl.when(before[1] & after[1])
        def _():
            @pl.when(before[2])
            def _():
                for copy in send_o3(i):
                    copy.wait_recv()

            h = lax.div(i, 2)
            for s in range(2):
                t = 2 * i + s
                g = t - h * G
                top, total, (p2,) = softmax_of([scores_of(rows_of(k1, h, g), rows_of(q1, t), bias2[...])])
                o = jnp.dot(v1t[h, :, tile(g)], p2, preferred_element_type=F32)
                lse = l3_in[t]
                peak = jnp.maximum(top, lse)
                here = jnp.exp2(top - peak)
                there = jnp.exp2(lse - peak)
                whole = total * here + there
                o1[t] = (o * (here / whole) + o3_in[t].astype(F32) * (there / whole)).astype(BF16)
                l1[t] = peak + jnp.log2(whole)
            for copy in send_o1(i):
                copy.start()

    def i32(i):
        return jnp.int32(i)

    def wide(i):
        widest(i32(i))
        extra(i32(i))

    def early(i):
        pl.when(after[2])(functools.partial(pass_on, i))

    with jax.named_scope("wide03"):
        context(0)
        wide(0)
        wide(1)
        context(1)
        wide(2)
        early(half)
        wide(3)
        early(half + 1)
    with jax.named_scope("local0"):
        local(0)
        early(half + 2)
        answer(i32(0))
    with jax.named_scope("local1"):
        local(1)
        early(half + 3)
        answer(i32(1))
        answer(i32(2))

        @pl.when(c + 2 == n)
        def _():
            for i in range(half, chunks):
                pass_on(i)

    with jax.named_scope("wide45"):
        context(2)
        wide(4)
        answer(i32(3))
        local(2)
        wide(5)
    with jax.named_scope("wide67"):
        context(3)
        wide(6)
        local(3)
        wide(7)

    def row_block(b):
        return slice(b * T, (b + 1) * T)

    def term(u, h, b):
        start = pl.multiple_of(u * width + h * HEAD, HEAD)
        return jnp.dot(mixed[u, h, row_block(b), :], wo_v[pl.ds(start, HEAD), :], preferred_element_type=F32)

    def finish(h):
        with jax.named_scope(f"head{h}"):
            @pl.when(before[2])
            def _():
                for i in (2 * h, 2 * h + 1):
                    for copy in send_o1(i):
                        copy.wait_recv()

            for g in range(G):
                t = h * G + g
                top, lse = loc_m[t], l1_in[t]
                peak = jnp.maximum(top, lse)
                here = jnp.exp2(top - peak)
                there = jnp.exp2(lse - peak)
                whole = loc_l[t] * here + there
                o = loc_o[t] * (here / whole) + o1_in[t].astype(F32) * (there / whole)
                mix_t[h, :, g * T:(g + 1) * T] = o.astype(BF16)
            mixed[tp, h] = lax.dot_general(perm_out[...], mix_t[h], NT, preferred_element_type=F32).astype(BF16)
            send_mixed(h).start()
        with jax.named_scope(f"acc{h}"):
            for b in range(G):
                y = term(tp, h, b)
                acc[row_block(b)] = y if h == 0 else acc[row_block(b)] + y
            if h < heads - 1:
                send_mixed(h).wait_recv()
                for b in range(G):
                    acc[row_block(b)] += term(1 - tp, h, b)

    load(4).wait()
    with jax.named_scope("final"):
        finish(0)
    with jax.named_scope("o1b"):
        for i in (half, half + 1):
            answer(jnp.int32(i))
    with jax.named_scope("finalb"):
        finish(1)
    with jax.named_scope("o1c"):
        for i in range(half + 2, chunks):
            answer(jnp.int32(i))
    with jax.named_scope("finalc"):
        for h in range(2, heads):
            finish(h)

    with jax.named_scope("out"):
        send_mixed(heads - 1).wait_recv()
        for b in range(G):
            out_v[row_block(b)] = (acc[row_block(b)] + term(1 - tp, heads - 1, b)).astype(BF16)
            send_out(b).start()

    with jax.named_scope("drain"):
        send_tokens().wait_send()

        @pl.when(after[1])
        def _():
            for h in range(heads):
                for u in range(2):
                    send_k(h, u).wait_send()
                    send_v(h, u).wait_send()

        @pl.loop(0, chunks)
        def _(i):
            @pl.when(before[2])
            def _():
                send_q1(i).wait_send()

            @pl.when(before[3] & after[1])
            def _():
                send_q3(i).wait_send()

            @pl.when((c == 2) & after[1])
            def _():
                send_qx(i).wait_send()

            @pl.when((c == 1) & after[2])
            def _():
                for copy in send_ox(i):
                    copy.wait_send()

            @pl.when(before[1] & after[3])
            def _():
                for copy in send_o3(i):
                    copy.wait_send()

            @pl.when(before[1] & after[1])
            def _():
                for copy in send_o1(i):
                    copy.wait_send()

        for h in range(heads):
            send_mixed(h).wait_send()
        for b in range(G):
            send_out(b).wait()


def body(tokens, query_weight, key_weight, value_weight, output_weight):
    n = lax.axis_size("sp")
    half_rows, depth = tokens.shape
    width = query_weight.shape[1]
    heads = width // HEAD
    tiles, chunks = heads * G, 2 * heads
    features = output_weight.shape[1]
    assert 2 * half_rows == ROWS and FAR_DILATION == MIDDLE_DILATION**2 and heads % 2 == 0
    assert output_weight.shape[0] == 2 * width
    vmem = pltpu.VMEM
    dma = pltpu.SemaphoreType.DMA
    split = (tiles, 2, T // 2, HEAD)
    by_head = (heads, G, 2, T // 2, HEAD)
    turned = (heads, HEAD, ROWS)
    square = (tiles, T, HEAD)
    stat = (tiles, 1, T)
    scratch = [
        vmem((2, half_rows, depth), BF16), vmem((2, half_rows, depth), BF16),
        vmem((depth, width), BF16), vmem((depth, width), BF16), vmem((depth, width), BF16),
        vmem((2 * width, features), BF16), vmem((ROWS, features), BF16), vmem((ROWS, features), F32),
        vmem((2, half_rows, HEAD), F32), vmem((2, half_rows, HEAD), F32),
        vmem((G, 2, ROWS, T), F32), vmem((T, T), F32), vmem((2, T, T), F32),
        vmem((half_rows, half_rows), BF16), vmem((ROWS, ROWS), BF16),
        vmem(split, BF16),
        vmem(by_head, BF16), vmem(by_head, BF16), vmem(by_head, BF16), vmem(by_head, BF16),
        vmem(turned, BF16), vmem(turned, BF16),
        vmem(split, BF16), vmem(split, BF16), vmem(split, BF16), vmem(square, BF16), vmem(stat, F32),
        vmem(square, BF16), vmem(stat, F32), vmem(square, BF16), vmem(stat, F32),
        vmem(square, BF16), vmem(stat, F32), vmem(square, BF16), vmem(stat, F32),
        vmem(square, F32), vmem(stat, F32), vmem(stat, F32),
        vmem(turned, BF16), vmem((2, heads, ROWS, HEAD), BF16),
        dma((5,)), dma((2, 1)), dma((2, chunks)), dma((2, chunks)), dma((2, chunks)), dma((2, chunks)),
        dma((2, chunks)), dma((2, chunks)), dma((2, chunks)), dma((2, chunks)), dma((2, chunks)), dma((2, chunks)), dma((2, heads)), dma((G,)),
    ]
    hbm = pl.BlockSpec(memory_space=pltpu.HBM)
    return pl.pallas_call(
        functools.partial(kernel, n),
        out_shape=jax.ShapeDtypeStruct((ROWS, features), BF16),
        in_specs=[hbm] * 5,
        out_specs=pl.BlockSpec(memory_space=pl.ANY),
        scratch_shapes=scratch,
        compiler_params=pltpu.CompilerParams(
            collective_id=0, has_side_effects=True, vmem_limit_bytes=VMEM_LIMIT),
        name="attention",
    )(tokens, query_weight, key_weight, value_weight, output_weight)


def solution(mesh):
    in_specs = (
        P(("grp", "sp", "tp"), None),
        P(None, "tp"),
        P(None, "tp"),
        P(None, "tp"),
        P(None, "tp"),
    )
    out_specs = P(("grp", "sp"), "tp")
    return jax.shard_map(body, mesh=mesh, in_specs=in_specs, out_specs=out_specs, check_vma=False)
```
